512 devices in a mesh: fs: 64 (over z, y), tp: 8 (over x, core).
Axes of the slice: x: 4, y: 8, z: 8, core: 2. Of those that a mesh axis runs over, the one named last changes fastest.
Arguments:
- tokens: bfloat16 [24576, 2048], P('fs', 'tp'), may hold values from -60 to 60
- gain_mixer: float32 [2048], P('tp'), may hold values from 0.1 to 1.9
- w_in: bfloat16 [2048, 1024], P('fs', 'tp'), may hold values from -0.125 to 0.125
- pool_scale: float32 [1024], P('tp'), may hold values from 0.1 to 1.9
- w_pool_out: bfloat16 [2048, 1024], P('fs', 'tp'), may hold values from -0.5 to 0.5
- gain_mid: float32 [2048], P('tp'), may hold values from 0.1 to 1.9
- w_ff1: bfloat16 [2048, 8192], P('fs', 'tp'), may hold values from -0.125 to 0.125
- w_ff2: bfloat16 [2048, 8192], P('fs', 'tp'), may hold values from -0.1875 to 0.1875
- gain_out: float32 [2048], P('tp'), may hold values from 0.1 to 1.9
Outputs:
- layer_out: bfloat16 [24576, 2048], P('fs', 'tp')
The draws below stay inside these ranges and needn't reach their ends.
All inputs are finite; a program needn't handle non-finite values.
Results may differ from the reference program's by a relative error of at most 0.017.
Values may be sent and summed in bfloat16 or wider, within the bound.
No kernel may reach another device: no remote copies, remote signals or barrier semaphores. Data moves between devices by JAX's collectives and lax.ppermute only.
A program may use at most 64 MiB of HBM per device.

```python
import math
import jax
import jax.numpy as jnp
from jax import lax

D = 2048
POOL_WIDTH = 1024
FF = 8192
SEQ_DEV = 384
TOKENS = 24576
N_FS = 64
N_TP = 8


def draw_tokens(key, part):
    key_values = jax.random.fold_in(key, 11)
    key_rough = jax.random.fold_in(key, 12)
    column = jnp.arange(D, dtype=jnp.float32) / D
    rough = jax.random.uniform(key_rough, (D,), jnp.float32, 0.6, 1.5)
    scale = jnp.exp(math.log(4.0) * column) * rough
    values = jnp.clip(jax.random.normal(key_values, (TOKENS, D), jnp.float32), -6.0, 6.0)
    return (values * scale).astype(jnp.bfloat16)


def spiked(values, own_key, source, target, shards_of, factor):
    def block_of(dim):
        return (jnp.arange(values.shape[dim]) // (values.shape[dim] // shards_of)).reshape((-1,) + (1,) * (values.ndim - 1 - dim))

    first = jax.random.permutation(own_key, shards_of)[block_of(target)]
    second = (block_of(target) + shards_of // 2) % shards_of
    return jnp.where((block_of(source) == first) | (block_of(source) == second), factor * values, values)


def block_scale(key, dims, shards, low, top_value):
    factor_of, own = 1.0, jax.random.fold_in(key, 6)
    for dim, blocks in shards:
        heights = jnp.exp(jax.random.uniform(jax.random.fold_in(own, dim), (blocks,), jnp.float32, low / len(shards), top_value / len(shards)))
        factor_of = factor_of * jnp.repeat(heights, dims[dim] // blocks).reshape([-1 if axis == dim else 1 for axis in range(len(dims))])
    return factor_of


def noise(key, extent, scale, reach, split=(), kind=jnp.bfloat16):
    level = block_scale(key, extent, split, -0.22, 0.18) if split else 1.0
    drawn = jax.random.normal(key, extent, jnp.float32) * scale * level
    return jnp.minimum(jnp.maximum(drawn, -reach), reach).astype(kind)


def noise_with(key, shape, scale, bound, cuts, heavy, held_as=jnp.bfloat16):
    entries = scale * jax.random.normal(key, shape, jnp.float32)
    if cuts:
        entries = entries * block_scale(key, shape, cuts, -0.22, 0.18)
    return jnp.clip(spiked(entries, jax.random.fold_in(key, 3), *heavy), -bound, bound).astype(held_as)


def setup_inputs(seed: int = 0) -> dict:
    splits = jax.random.split(jax.random.key(seed), 10)
    return {
        "tokens": draw_tokens(jax.random.fold_in(splits[9], 71), 0),
        "gain_mixer": jnp.clip(1.0 + 0.18 * jax.random.normal(splits[1], (D,), jnp.float32), 0.1, 1.9),
        "w_in": noise(splits[2], (D, POOL_WIDTH), D ** -0.5, 0.125, ((0, 64), (1, 8))),
        "pool_scale": jnp.clip(1.0 + 0.18 * jax.random.normal(splits[3], (POOL_WIDTH,), jnp.float32), 0.1, 1.9),
        "w_pool_out": noise_with(splits[4], (D, POOL_WIDTH), POOL_WIDTH ** -0.5, 0.5, ((0, 64), (1, 8)), (1, 0, 64, 4.0)),
        "gain_mid": jnp.clip(1.0 + 0.18 * jax.random.normal(splits[5], (D,), jnp.float32), 0.1, 1.9),
        "w_ff1": noise(splits[6], (D, FF), D ** -0.5, 0.125, ((0, 64), (1, 8))),
        "w_ff2": noise_with(splits[7], (D, FF), FF ** -0.5, 0.1875, ((0, 64), (1, 8)), (1, 0, 64, 4.0)),
        "gain_out": jnp.clip(1.0 + 0.18 * jax.random.normal(splits[8], (D,), jnp.float32), 0.1, 1.9),
    }


norm_eps = 1e-05
residual_alpha = 2.0 ** 0.25

def norm_rows(value, gain):
    center = value - lax.optimization_barrier(jnp.mean(value, axis=-1, keepdims=True))
    spread = lax.optimization_barrier(jnp.mean(center * center, axis=-1, keepdims=True))
    return center * lax.rsqrt(spread + norm_eps) * gain

def block_sums(left, weight, blocks):
    width = left.shape[1] // blocks
    total = jnp.zeros((left.shape[0], weight.shape[0]), jnp.float32)
    for block in range(blocks):
        term = lax.dot_general(left[:, block * width:(block + 1) * width], weight[:, block * width:(block + 1) * width], (((1,), (1,)), ((), ())), preferred_element_type=jnp.float32)
        term = lax.optimization_barrier(term.astype(jnp.bfloat16))
        total = total + term.astype(jnp.float32)
    return total.astype(jnp.bfloat16)

def reference(tokens, gain_mixer, w_in, pool_scale, w_pool_out, gain_mid, w_ff1, w_ff2, gain_out):
    group = POOL_WIDTH // 4

    def one_sequence(seq_rows):
        xf = seq_rows.astype(jnp.float32)
        mixed_in = norm_rows(xf, gain_mixer).astype(jnp.bfloat16)
        pool_in = jnp.dot(mixed_in, w_in, preferred_element_type=jnp.float32).astype(jnp.bfloat16)
        uf = pool_in.astype(jnp.float32)
        length = uf.shape[0]
        sums = jnp.pad(jnp.cumsum(uf, axis=0), ((1, 0), (0, 0)))
        position = jnp.arange(length, dtype=jnp.float32)[:, None]
        pieces = []
        for index, window in enumerate((2, 4, 8, 16)):
            part = sums[:, index * group:(index + 1) * group]
            upper = part[1:]
            lower = jnp.pad(part, ((window - 1, 0), (0, 0)))[:length]
            count = jnp.minimum(position + 1.0, float(window))
            pieces.append((upper - lower) / count - uf[:, index * group:(index + 1) * group])
        pooled = (jnp.concatenate(pieces, axis=1) * pool_scale).astype(jnp.bfloat16)
        mixer_out = block_sums(pooled, w_pool_out, N_TP)
        middle = norm_rows(residual_alpha * xf + mixer_out.astype(jnp.float32), gain_mid).astype(jnp.bfloat16)
        upward = jnp.dot(middle, w_ff1, preferred_element_type=jnp.float32)
        hidden = jnp.square(jax.nn.relu(upward)).astype(jnp.bfloat16)
        ff_out = block_sums(hidden, w_ff2, N_TP)
        result = norm_rows(residual_alpha * middle.astype(jnp.float32) + ff_out.astype(jnp.float32), gain_out)
        return result.astype(jnp.bfloat16)
    stacked = tokens.reshape(N_FS, SEQ_DEV, D)
    return lax.map(one_sequence, stacked).reshape(N_FS * SEQ_DEV, D)
```

```python
import functools

import jax
import jax.numpy as jnp
from jax import lax
from jax.experimental import pallas as pl
from jax.experimental.pallas import tpu as pltpu
from jax.sharding import Mesh, PartitionSpec as P

norm_eps = 1e-05
residual_alpha = 2.0**0.25
FS = ("z", "y")
TP = ("x", "core")
bf16 = jnp.bfloat16
f32 = jnp.float32
VMEM_LIMIT = 60 * 1024 * 1024


def everyone(array, axis):
    count = lax.axis_size(axis)
    return lax.all_to_all(
        jnp.broadcast_to(array[None], (count, *array.shape)), axis, 0, 0, tiled=True
    )


def gather_tp(piece):
    return everyone(everyone(piece, "x"), "core")


def scatter_sum_tp(parts):
    both = lax.all_to_all(parts, "core", 0, 0, tiled=True).astype(f32)
    chip = (both[0] + both[1]).astype(bf16)
    four = lax.all_to_all(chip, "x", 0, 0, tiled=True).astype(f32)
    return (four[0] + four[1]) + (four[2] + four[3])


def row_statistics(load, blocks, width):
    total = None
    for b in range(blocks):
        s = jnp.sum(load(b), axis=1, keepdims=True)
        total = s if total is None else total + s
    mean = total / width
    spread = None
    for b in range(blocks):
        c = load(b) - mean
        s = jnp.sum(c * c, axis=1, keepdims=True)
        spread = s if spread is None else spread + s
    return mean, lax.rsqrt(spread / width + norm_eps)


def shift_down(value, steps, row):
    return jnp.where(row >= steps, pltpu.roll(value, steps, 0), 0.0)


def mixer_kernel(rows, tok_ref, gain_ref, w_in_ref, w_out_ref, scale_ref, out_ref, mixed_ref):
    tiles = 3
    step = rows // tiles
    for t in range(tiles):
        part = pl.ds(t * step, step)
        load = lambda b: tok_ref[b % 2, b // 2, part, :].astype(f32)
        mean, inverse = row_statistics(load, 8, 2048)
        for b in range(8):
            columns = slice(b * 256, (b + 1) * 256)
            mixed = (load(b) - mean) * inverse * gain_ref[:, columns]
            mixed_ref[part, columns] = mixed.astype(bf16)
    pool_in = jnp.dot(mixed_ref[...], w_in_ref[...], preferred_element_type=f32)
    u = pool_in.astype(bf16).astype(f32)
    row = lax.broadcasted_iota(jnp.int32, u.shape, 0)
    group = lax.axis_index("x")
    two = u + shift_down(u, 1, row)
    four = two + shift_down(two, 2, row)
    eight = four + shift_down(four, 4, row)
    sixteen = eight + shift_down(eight, 8, row)
    total = jnp.where(
        group == 0, two, jnp.where(group == 1, four, jnp.where(group == 2, eight, sixteen))
    )
    window = jnp.where(group == 0, 2, jnp.where(group == 1, 4, jnp.where(group == 2, 8, 16)))
    count = jnp.minimum(row + 1, window).astype(f32)
    pooled = ((total / count - u) * scale_ref[...]).astype(bf16)
    for b in range(8):
        rows_out = w_out_ref[b * 256 : (b + 1) * 256, :]
        term = lax.dot_general(
            pooled, rows_out, (((1,), (1,)), ((), ())), preferred_element_type=f32
        )
        out_ref[b % 2, b // 2] = term.astype(bf16)


def ff_kernel(
    rows, tok_ref, mix_ref, gain_ref, w_ref, out_ref, own_ref, mid_ref, hid_ref, w_vmem, sems
):
    pieces = 8
    depth = 2048 // pieces
    copies = []
    for half in range(2):
        for p in range(pieces):
            where = (pl.ds(p * depth, depth), pl.ds(half * 1024, 1024))
            copy = pltpu.make_async_copy(
                w_ref.at[where], w_vmem.at[half, pl.ds(p * depth, depth)], sems.at[half, p]
            )
            copy.start()
            copies.append(copy)
    tiles = 3
    step = rows // tiles
    for t in range(tiles):
        part = pl.ds(t * step, step)
        load = lambda b: residual_alpha * tok_ref[b % 2, b // 2, part, :].astype(f32) + mix_ref[
            b % 2, b // 2, part, :
        ].astype(f32)
        mean, inverse = row_statistics(load, 8, 2048)
        for b in range(8):
            columns = slice(b * 256, (b + 1) * 256)
            mid = (load(b) - mean) * inverse * gain_ref[:, columns]
            mid_ref[b % 2, b // 2, part, :] = mid.astype(bf16)
    own_ref[...] = mid_ref[lax.axis_index("core"), lax.axis_index("x")]
    up = None
    for p in range(pieces):
        copies[p].wait()
        term = jnp.dot(mid_ref[p % 2, p // 2], w_vmem[0, pl.ds(p * depth, depth), :],
                       preferred_element_type=f32)
        up = term if up is None else up + term
    up = jnp.maximum(up, 0.0)
    hid_ref[...] = (up * up).astype(bf16)
    for p in range(pieces):
        copies[pieces + p].wait()
        term = lax.dot_general(
            hid_ref[...],
            w_vmem[1, pl.ds(p * depth, depth), :],
            (((1,), (1,)), ((), ())),
            preferred_element_type=f32,
        )
        out_ref[p % 2, p // 2] = term.astype(bf16)


def vmem(count):
    return [pl.BlockSpec(memory_space=pltpu.VMEM)] * count


def local(tokens, gain_mixer, w_in, pool_scale, w_pool_out, gain_mid, w_ff1, w_ff2, gain_out):
    rows, width = tokens.shape
    channels = w_in.shape[1]
    ff_full = lax.all_gather(jnp.concatenate([w_ff1, w_ff2], axis=1), FS, axis=0, tiled=True)
    small = everyone(jnp.concatenate([w_in, w_pool_out], axis=1), FS).reshape(-1, 2 * channels)
    gains = everyone(jnp.stack([gain_mixer, gain_mid]), TP)
    gains = jnp.moveaxis(gains, 0, 1).reshape(2, 1, 8 * width)
    everything = gather_tp(tokens).reshape(2, 4, rows, width)
    parts = pl.pallas_call(
        functools.partial(mixer_kernel, rows),
        out_shape=jax.ShapeDtypeStruct((2, 4, rows, width), bf16),
        in_specs=vmem(5),
        out_specs=pl.BlockSpec(memory_space=pltpu.VMEM),
        scratch_shapes=[pltpu.VMEM((rows, 8 * width), bf16)],
        compiler_params=pltpu.CompilerParams(vmem_limit_bytes=24 * 1024 * 1024),
        cost_estimate=pl.CostEstimate(flops=4_000_000_000, bytes_accessed=4_000_000, transcendentals=0),
        name="mixer",
    )(everything, gains[0], small[:, :channels], small[:, channels:], pool_scale[None])
    mixer_out = scatter_sum_tp(parts).astype(bf16)
    mixed = gather_tp(mixer_out).reshape(2, 4, rows, width)
    parts, middle = pl.pallas_call(
        functools.partial(ff_kernel, rows),
        out_shape=(
            jax.ShapeDtypeStruct((2, 4, rows, width), bf16),
            jax.ShapeDtypeStruct((rows, width), bf16),
        ),
        in_specs=vmem(3) + [pl.BlockSpec(memory_space=pl.ANY)],
        out_specs=tuple(vmem(2)),
        scratch_shapes=[
            pltpu.VMEM((2, 4, rows, width), bf16),
            pltpu.VMEM((rows, 1024), bf16),
            pltpu.VMEM((2, 2048, 1024), bf16),
            pltpu.SemaphoreType.DMA((2, 8)),
        ],
        compiler_params=pltpu.CompilerParams(vmem_limit_bytes=40 * 1024 * 1024),
        cost_estimate=pl.CostEstimate(flops=8_000_000_000, bytes_accessed=12_000_000, transcendentals=0),
        name="feed_forward",
    )(everything, mixed, gains[1], ff_full)
    ff_out = scatter_sum_tp(parts).astype(bf16)
    value = residual_alpha * middle.astype(f32) + ff_out.astype(f32)
    part_mean = jnp.sum(value, axis=1) / width
    center = value - part_mean[:, None]
    part_spread = jnp.sum(center * center, axis=1)
    packed = jnp.concatenate([part_mean, part_spread])[None]
    means, spreads = jnp.split(everyone(packed, TP)[:, 0], 2, axis=1)
    mean = jnp.mean(means, axis=0)
    away = means - mean
    spread = (jnp.sum(spreads, axis=0) + width * jnp.sum(away * away, axis=0)) / (8 * width)
    result = (value - mean[:, None]) * lax.rsqrt(spread + norm_eps)[:, None] * gain_out
    return result.astype(bf16)


def solution(mesh):
    mesh = Mesh(mesh.devices.reshape(8, 8, 4, 2), FS + TP)
    return jax.shard_map(
        local,
        mesh=mesh,
        in_specs=(
            P(FS, TP),
            P(TP),
            P(FS, TP),
            P(TP),
            P(FS, TP),
            P(TP),
            P(FS, TP),
            P(FS, TP),
            P(TP),
        ),
        out_specs=P(FS, TP),
        check_vma=False,
    )
```

```python
import functools

import jax
import jax.numpy as jnp
from jax import lax
from jax.experimental import pallas as pl
from jax.experimental.pallas import tpu as pltpu
from jax.sharding import Mesh, PartitionSpec as P

norm_eps = 1e-05
residual_alpha = 2.0**0.25
FS = ("z", "y")
TP = ("x", "core")
bf16 = jnp.bfloat16
f32 = jnp.float32
EVERY = FS + TP


def device(z, y, x, core):
    return (((z % 8) * 8 + y % 8) * 4 + x) * 2 + core


PLACES = [(z, y, x) for z in range(8) for y in range(8) for x in range(4)]
FIRST = [[device(z, y, x, 0) for z in range(8)] for y in range(8) for x in range(4)] + [
    [device(z, y, x, 1) for y in range(8)] for z in range(8) for x in range(4)
]
SECOND = [[device(z, y, x, 0) for y in range(8)] for z in range(8) for x in range(4)] + [
    [device(z, y, x, 1) for z in range(8)] for y in range(8) for x in range(4)
]


def around(steps):
    return [
        pair
        for z, y, x in PLACES
        for pair in (
            (device(z, y, x, 0), device(z, y + steps, x, 0)),
            (device(z, y, x, 1), device(z + steps, y, x, 1)),
        )
    ]


def among(array, groups):
    return lax.all_to_all(
        jnp.broadcast_to(array[None], (8, *array.shape)),
        EVERY,
        0,
        0,
        axis_index_groups=groups,
        tiled=True,
    )


def everyone(array, axis):
    count = lax.axis_size(axis)
    return lax.all_to_all(
        jnp.broadcast_to(array[None], (count, *array.shape)), axis, 0, 0, tiled=True
    )


def gather_tp(piece):
    return everyone(everyone(piece, "x"), "core")


def scatter_sum_tp(parts):
    both = lax.all_to_all(parts, "core", 0, 0, tiled=True).astype(f32)
    chip = (both[0] + both[1]).astype(bf16)
    four = lax.all_to_all(chip, "x", 0, 0, tiled=True).astype(f32)
    return (four[0] + four[1]) + (four[2] + four[3])


def row_statistics(load, blocks, width):
    total = None
    for b in range(blocks):
        s = jnp.sum(load(b), axis=1, keepdims=True)
        total = s if total is None else total + s
    mean = total / width
    spread = None
    for b in range(blocks):
        c = load(b) - mean
        s = jnp.sum(c * c, axis=1, keepdims=True)
        spread = s if spread is None else spread + s
    return mean, lax.rsqrt(spread / width + norm_eps)


def shift_down(value, steps, row):
    return jnp.where(row >= steps, pltpu.roll(value, steps, 0), 0.0)


def gain_of(tok_ref, rows, b, first):
    parts = tok_ref[b % 2, b // 2, pl.ds(rows, 16), :].astype(f32)
    return parts[first : first + 1] + parts[first + 1 : first + 2] + parts[first + 2 : first + 3]


def mixer_kernel(rows, tok_ref, small_ref, scale_ref, out_ref, mixed_ref, w_ref):
    core = lax.axis_index("core")
    for s in range(8):
        for j in range(8):
            at = jnp.where(core == 0, j * 256 + s * 32, s * 256 + j * 32)
            w_ref[pl.ds(pl.multiple_of(at, 32), 32), :] = small_ref[s, j]
    tiles = 3
    step = rows // tiles
    for t in range(tiles):
        part = pl.ds(t * step, step)
        load = lambda b: tok_ref[b % 2, b // 2, part, :].astype(f32)
        mean, inverse = row_statistics(load, 8, 2048)
        for b in range(8):
            columns = slice(b * 256, (b + 1) * 256)
            mixed = (load(b) - mean) * inverse * gain_of(tok_ref, rows, b, 0)
            mixed_ref[part, columns] = mixed.astype(bf16)
    pool_in = jnp.dot(mixed_ref[...], w_ref[:, :128], preferred_element_type=f32)
    u = pool_in.astype(bf16).astype(f32)
    row = lax.broadcasted_iota(jnp.int32, u.shape, 0)
    group = lax.axis_index("x")
    two = u + shift_down(u, 1, row)
    four = two + shift_down(two, 2, row)
    eight = four + shift_down(four, 4, row)
    sixteen = eight + shift_down(eight, 8, row)
    total = jnp.where(
        group == 0, two, jnp.where(group == 1, four, jnp.where(group == 2, eight, sixteen))
    )
    window = jnp.where(group == 0, 2, jnp.where(group == 1, 4, jnp.where(group == 2, 8, 16)))
    count = jnp.minimum(row + 1, window).astype(f32)
    pooled = ((total / count - u) * scale_ref[...]).astype(bf16)
    for b in range(8):
        rows_out = w_ref[b * 256 : (b + 1) * 256, 128:]
        term = lax.dot_general(
            pooled, rows_out, (((1,), (1,)), ((), ())), preferred_element_type=f32
        )
        out_ref[b % 2, b // 2] = term.astype(bf16)


def ff_kernel(rows, tok_ref, mix_ref, *refs):
    chunks, (out_ref, own_ref, mid_ref, hid_ref, w_vmem, sems) = refs[:8], refs[8:]
    core = lax.axis_index("core")
    place = jnp.where(core == 0, lax.axis_index("y"), lax.axis_index("z"))
    copies = []
    for k, (chunk, offset) in enumerate(zip(chunks, OFFSETS)):
        source = lax.rem(place + (8 - offset), 8)
        for j in range(8):
            at = jnp.where(core == 0, j * 256 + source * 32, source * 256 + j * 32)
            copy = pltpu.make_async_copy(
                chunk.at[j], w_vmem.at[pl.ds(pl.multiple_of(at, 32), 32)], sems.at[k, j]
            )
            copy.start()
            copies.append(copy)
    tiles = 3
    step = rows // tiles
    for t in range(tiles):
        part = pl.ds(t * step, step)
        load = lambda b: residual_alpha * tok_ref[b % 2, b // 2, part, :].astype(f32) + mix_ref[
            b % 2, b // 2, part, :
        ].astype(f32)
        mean, inverse = row_statistics(load, 8, 2048)
        for b in range(8):
            mid = (load(b) - mean) * inverse * gain_of(tok_ref, rows, b, 3)
            mid_ref[b % 2, b // 2, part, :] = mid.astype(bf16)
    own_ref[...] = mid_ref[lax.axis_index("core"), lax.axis_index("x")]
    for copy in copies:
        copy.wait()
    up = None
    for b in range(8):
        term = jnp.dot(
            mid_ref[b % 2, b // 2],
            w_vmem[b * 256 : (b + 1) * 256, :1024],
            preferred_element_type=f32,
        )
        up = term if up is None else up + term
    up = jnp.maximum(up, 0.0)
    hid_ref[...] = (up * up).astype(bf16)
    for b in range(8):
        term = lax.dot_general(
            hid_ref[...],
            w_vmem[b * 256 : (b + 1) * 256, 1024:],
            (((1,), (1,)), ((), ())),
            preferred_element_type=f32,
        )
        out_ref[b % 2, b // 2] = term.astype(bf16)


OFFSETS = (0, 1, -1, 2, -2, 3, -3, 4)


def in_three(gain):
    rest, rows = gain, []
    for _ in range(3):
        rows.append(lax.reduce_precision(rest, 8, 7))
        rest = rest - rows[-1]
    return jnp.stack(rows).astype(bf16)


def vmem(count):
    return [pl.BlockSpec(memory_space=pltpu.VMEM)] * count


def local(tokens, gain_mixer, w_in, pool_scale, w_pool_out, gain_mid, w_ff1, w_ff2, gain_out):
    rows, width = tokens.shape
    channels = w_in.shape[1]
    packed = jnp.concatenate([w_ff1, w_ff2, w_in, w_pool_out], axis=1)
    first = among(packed, FIRST)
    small = among(first[:, :, 2048:].reshape(256, 2 * channels), SECOND)
    small = small.reshape(8, 8, 32, 2 * channels)
    chunk = first[:, :, :2048]
    chunks = [chunk]
    up, down = chunk, chunk
    for hop in range(4):
        up = lax.ppermute(up, EVERY, around(1))
        chunks.append(up)
        if hop < 3:
            down = lax.ppermute(down, EVERY, around(-1))
            chunks.append(down)
    everything = gather_tp(
        jnp.concatenate([tokens, in_three(gain_mixer), in_three(gain_mid), jnp.zeros((10, width), bf16)])
    )
    parts = pl.pallas_call(
        functools.partial(mixer_kernel, rows),
        out_shape=jax.ShapeDtypeStruct((2, 4, rows, width), bf16),
        in_specs=vmem(3),
        out_specs=pl.BlockSpec(memory_space=pltpu.VMEM),
        scratch_shapes=[
            pltpu.VMEM((rows, 8 * width), bf16),
            pltpu.VMEM((8 * width, 2 * channels), bf16),
        ],
        compiler_params=pltpu.CompilerParams(vmem_limit_bytes=24 * 1024 * 1024),
        cost_estimate=pl.CostEstimate(flops=4_000_000_000, bytes_accessed=4_000_000, transcendentals=0),
        name="mixer",
    )(everything, small, pool_scale[None])
    mixer_out = scatter_sum_tp(parts).astype(bf16)
    mixed = gather_tp(mixer_out)
    parts, middle = pl.pallas_call(
        functools.partial(ff_kernel, rows),
        out_shape=(
            jax.ShapeDtypeStruct((2, 4, rows, width), bf16),
            jax.ShapeDtypeStruct((rows, width), bf16),
        ),
        in_specs=vmem(2) + [pl.BlockSpec(memory_space=pl.ANY)] * 8,
        out_specs=tuple(vmem(2)),
        scratch_shapes=[
            pltpu.VMEM((2, 4, rows, width), bf16),
            pltpu.VMEM((rows, 1024), bf16),
            pltpu.VMEM((2048, 2048), bf16),
            pltpu.SemaphoreType.DMA((8, 8)),
        ],
        compiler_params=pltpu.CompilerParams(vmem_limit_bytes=30 * 1024 * 1024),
        cost_estimate=pl.CostEstimate(flops=8_000_000_000, bytes_accessed=12_000_000, transcendentals=0),
        name="feed_forward",
    )(everything, mixed, *chunks)
    ff_out = scatter_sum_tp(parts).astype(bf16)
    value = residual_alpha * middle.astype(f32) + ff_out.astype(f32)
    part_mean = jnp.sum(value, axis=1) / width
    center = value - part_mean[:, None]
    part_spread = jnp.sum(center * center, axis=1)
    packed = jnp.concatenate([part_mean, part_spread])[None]
    means, spreads = jnp.split(everyone(packed, TP)[:, 0], 2, axis=1)
    mean = jnp.mean(means, axis=0)
    away = means - mean
    spread = (jnp.sum(spreads, axis=0) + width * jnp.sum(away * away, axis=0)) / (8 * width)
    result = (value - mean[:, None]) * lax.rsqrt(spread + norm_eps)[:, None] * gain_out
    return result.astype(bf16)


def solution(mesh):
    mesh = Mesh(mesh.devices.reshape(8, 8, 4, 2), FS + TP)
    return jax.shard_map(
        local,
        mesh=mesh,
        in_specs=(
            P(FS, TP),
            P(TP),
            P(FS, TP),
            P(TP),
            P(FS, TP),
            P(TP),
            P(FS, TP),
            P(FS, TP),
            P(TP),
        ),
        out_specs=P(FS, TP),
        check_vma=False,
    )
```

```python
import functools

import jax
import jax.numpy as jnp
from jax import lax
from jax.experimental import pallas as pl
from jax.experimental.pallas import tpu as pltpu
from jax.sharding import Mesh, PartitionSpec as P


norm_eps = 1e-05
residual_alpha = 2.0**0.25
FS = ("z", "y")
TP = ("x", "core")
EVERY = FS + TP
bf16 = jnp.bfloat16
f32 = jnp.float32
OFFSETS = (0, 1, -1, 2, -2, 3, -3, 4)
MEBI = 1024 * 1024


def device(z, y, x, core):
    return (((z % 8) * 8 + y % 8) * 4 + x % 4) * 2 + core % 2


PLACES = [(z, y, x) for z in range(8) for y in range(8) for x in range(4)]
FIRST = [[device(z, y, x, 0) for z in range(8)] for y in range(8) for x in range(4)] + [
    [device(z, y, x, 1) for y in range(8)] for z in range(8) for x in range(4)
]
SECOND = [[device(z, y, x, 0) for y in range(8)] for z in range(8) for x in range(4)] + [
    [device(z, y, x, 1) for z in range(8)] for y in range(8) for x in range(4)
]


def around(steps):
    return [
        pair
        for z, y, x in PLACES
        for pair in (
            (device(z, y, x, 0), device(z, y + steps, x, 0)),
            (device(z, y, x, 1), device(z + steps, y, x, 1)),
        )
    ]


def along_x(array, steps):
    pairs = [
        (device(z, y, x, c), device(z, y, x + steps, c)) for z, y, x in PLACES for c in range(2)
    ]
    return lax.ppermute(array, EVERY, pairs)


def from_other_core(array):
    return lax.ppermute(array, "core", [(0, 1), (1, 0)])


def everyone(array, axis):
    count = lax.axis_size(axis)
    return lax.all_to_all(
        jnp.broadcast_to(array[None], (count, *array.shape)), axis, 0, 0, tiled=True
    )


def among(array, groups):
    return lax.all_to_all(
        jnp.broadcast_to(array[None], (8, *array.shape)),
        EVERY,
        0,
        0,
        axis_index_groups=groups,
        tiled=True,
    )


def scatter_sum_tp(keep, send):
    chip = (keep.astype(f32) + from_other_core(send).astype(f32)).astype(bf16)
    four = lax.all_to_all(chip, "x", 0, 0, tiled=True).astype(f32)
    return (four[0] + four[1]) + (four[2] + four[3])


def in_three(gain):
    rest, rows = gain, []
    for _ in range(3):
        rows.append(lax.reduce_precision(rest, 8, 7))
        rest = rest - rows[-1]
    return jnp.stack(rows).astype(bf16)


def gain_of(tok_ref, block, rows, first):
    parts = tok_ref[block, pl.ds(rows, 16), :].astype(f32)
    return parts[first : first + 1] + parts[first + 1 : first + 2] + parts[first + 2 : first + 3]


def columns_of(x, core):
    return pl.ds(pl.multiple_of((2 * x + core) * 256, 256), 256)


def row_at(core, source, j):
    at = jnp.where(core == 0, j * 256 + source * 32, source * 256 + j * 32)
    return pl.ds(pl.multiple_of(at, 32), 32)


def row_statistics(loads, width):
    total = None
    for load in loads:
        s = jnp.sum(load(), axis=1, keepdims=True)
        total = s if total is None else total + s
    mean = total / width
    spread = None
    for load in loads:
        c = load() - mean
        s = jnp.sum(c * c, axis=1, keepdims=True)
        spread = s if spread is None else spread + s
    return mean, lax.rsqrt(spread / width + norm_eps)


def shift_down(value, steps, row):
    return jnp.where(row >= steps, pltpu.roll(value, steps, 0), 0.0)


def mixer_kernel(rows, mine_ref, other_ref, small_ref, scale_ref, keep_ref, send_ref, mixed_ref, w_ref):
    x, core = lax.axis_index("x"), lax.axis_index("core")
    for s in range(8):
        for j in range(8):
            w_ref[row_at(core, s, j), :] = small_ref[s, j]
    step = rows // 3
    for t in range(3):
        part = pl.ds(t * step, step)
        blocks = [(ref, r) for ref in (mine_ref, other_ref) for r in range(4)]
        loads = [lambda ref=ref, r=r: ref[r, part, :].astype(f32) for ref, r in blocks]
        mean, inverse = row_statistics(loads, 2048)
        for (ref, r), load in zip(blocks, loads):
            where = columns_of(lax.rem(x + (4 - r), 4), core if ref is mine_ref else 1 - core)
            mixed = (load() - mean) * inverse * gain_of(ref, r, rows, 0)
            mixed_ref[part, where] = mixed.astype(bf16)
    pool_in = jnp.dot(mixed_ref[...], w_ref[:, :128], preferred_element_type=f32)
    u = pool_in.astype(bf16).astype(f32)
    row = lax.broadcasted_iota(jnp.int32, u.shape, 0)
    two = u + shift_down(u, 1, row)
    four = two + shift_down(two, 2, row)
    eight = four + shift_down(four, 4, row)
    sixteen = eight + shift_down(eight, 8, row)
    total = jnp.where(x == 0, two, jnp.where(x == 1, four, jnp.where(x == 2, eight, sixteen)))
    window = jnp.where(x == 0, 2, jnp.where(x == 1, 4, jnp.where(x == 2, 8, 16)))
    count = jnp.minimum(row + 1, window).astype(f32)
    pooled = ((total / count - u) * scale_ref[...]).astype(bf16)
    for xb in range(4):
        for ref, c in ((keep_ref, core), (send_ref, 1 - core)):
            term = lax.dot_general(
                pooled,
                w_ref[columns_of(xb, c), 128:],
                (((1,), (1,)), ((), ())),
                preferred_element_type=f32,
            )
            ref[xb] = term.astype(bf16)


def ff_kernel(rows, mine_ref, other_ref, mix_ref, mix_other_ref, *refs):
    chunks, (keep_ref, send_ref, own_ref, mid_ref, hid_ref, w_ref, sems) = refs[:8], refs[8:]
    x, core = lax.axis_index("x"), lax.axis_index("core")
    place = jnp.where(core == 0, lax.axis_index("y"), lax.axis_index("z"))
    copies = []
    for k, (chunk, offset) in enumerate(zip(chunks, OFFSETS)):
        source = lax.rem(place + (8 - offset), 8)
        for j in range(8):
            copy = pltpu.make_async_copy(
                chunk.at[j], w_ref.at[row_at(core, source, j)], sems.at[k, j]
            )
            copy.start()
            copies.append(copy)
    step = rows // 3
    for t in range(3):
        part = pl.ds(t * step, step)
        blocks = [
            (tok, mix, c, xb)
            for tok, mix, c in ((mine_ref, mix_ref, core), (other_ref, mix_other_ref, 1 - core))
            for xb in range(4)
        ]

        def total(tok, mix, xb):
            r = lax.rem(x + (4 - xb), 4)
            return residual_alpha * tok[r, part, :].astype(f32) + mix[xb, part, :].astype(f32)

        loads = [functools.partial(total, tok, mix, xb) for tok, mix, _, xb in blocks]
        mean, inverse = row_statistics(loads, 2048)
        for (tok, mix, c, xb), load in zip(blocks, loads):
            gain = gain_of(tok, lax.rem(x + (4 - xb), 4), rows, 3)
            mid_ref[part, columns_of(xb, c)] = ((load() - mean) * inverse * gain).astype(bf16)
    own_ref[...] = mid_ref[:, columns_of(x, core)]
    for copy in copies:
        copy.wait()
    for n in range(4):
        where = slice(n * 256, (n + 1) * 256)
        up = jnp.dot(mid_ref[...], w_ref[:, where], preferred_element_type=f32)
        up = jnp.maximum(up, 0.0)
        hid_ref[:, where] = (up * up).astype(bf16)
    for xb in range(4):
        for ref, c in ((keep_ref, core), (send_ref, 1 - core)):
            term = lax.dot_general(
                hid_ref[...],
                w_ref[columns_of(xb, c), 1024:],
                (((1,), (1,)), ((), ())),
                preferred_element_type=f32,
            )
            ref[xb] = term.astype(bf16)


def vmem(count):
    return [pl.BlockSpec(memory_space=pltpu.VMEM)] * count


def mixer(mine, other, small, scale, rows, width, channels):
    block = jax.ShapeDtypeStruct((4, rows, width), bf16)
    return pl.pallas_call(
        functools.partial(mixer_kernel, rows),
        out_shape=(block, block),
        in_specs=vmem(4),
        out_specs=tuple(vmem(2)),
        scratch_shapes=[
            pltpu.VMEM((rows, 8 * width), bf16),
            pltpu.VMEM((8 * width, 2 * channels), bf16),
        ],
        compiler_params=pltpu.CompilerParams(vmem_limit_bytes=24 * MEBI),
        cost_estimate=pl.CostEstimate(flops=4_000_000_000, bytes_accessed=4_000_000, transcendentals=0),
        name="mixer",
    )(mine, other, small, scale)


def feed_forward(mine, other, mix, mix_other, chunks, rows, width):
    block = jax.ShapeDtypeStruct((4, rows, width), bf16)
    return pl.pallas_call(
        functools.partial(ff_kernel, rows),
        out_shape=(block, block, jax.ShapeDtypeStruct((rows, width), bf16)),
        in_specs=vmem(4) + [pl.BlockSpec(memory_space=pl.ANY)] * 8,
        out_specs=tuple(vmem(3)),
        scratch_shapes=[
            pltpu.VMEM((rows, 8 * width), bf16),
            pltpu.VMEM((rows, 1024), bf16),
            pltpu.VMEM((2048, 2048), bf16),
            pltpu.SemaphoreType.DMA((8, 8)),
        ],
        compiler_params=pltpu.CompilerParams(vmem_limit_bytes=30 * MEBI),
        cost_estimate=pl.CostEstimate(flops=8_000_000_000, bytes_accessed=12_000_000, transcendentals=0),
        name="feed_forward",
    )(mine, other, mix, mix_other, *chunks)


def layer(tokens, gain_mixer, w_in, pool_scale, w_pool_out, gain_mid, w_ff1, w_ff2, gain_out):
    rows, width = tokens.shape
    channels = w_in.shape[1]
    packed = jnp.concatenate([w_ff1, w_ff2, w_in, w_pool_out], axis=1)
    first = among(packed, FIRST)
    small = among(first[:, :, 2048:].reshape(256, 2 * channels), SECOND)
    small = small.reshape(8, 8, 32, 2 * channels)
    chunk = first[:, :, :2048]
    chunks = [chunk]
    up, down = chunk, chunk
    for hop in range(4):
        up = lax.ppermute(up, EVERY, around(1))
        chunks.append(up)
        if hop < 3:
            down = lax.ppermute(down, EVERY, around(-1))
            chunks.append(down)
    extended = jnp.concatenate(
        [tokens, in_three(gain_mixer), in_three(gain_mid), jnp.zeros((10, width), bf16)]
    )
    pieces = [extended]
    for steps in (1, 2, 3):
        pieces.append(along_x(extended, steps))
    mine = jnp.stack(pieces)
    other = from_other_core(mine)
    keep, send = mixer(mine, other, small, pool_scale[None], rows, width, channels)
    mixer_out = scatter_sum_tp(keep, send).astype(bf16)
    mix = everyone(mixer_out, "x")
    mix_other = from_other_core(mix)
    keep, send, middle = feed_forward(mine, other, mix, mix_other, chunks, rows, width)
    ff_out = scatter_sum_tp(keep, send).astype(bf16)
    value = residual_alpha * middle.astype(f32) + ff_out.astype(f32)
    part_mean = jnp.sum(value, axis=1) / width
    center = value - part_mean[:, None]
    part_spread = jnp.sum(center * center, axis=1)
    sums = jnp.concatenate([part_mean, part_spread])[None]
    means, spreads = jnp.split(everyone(sums, TP)[:, 0], 2, axis=1)
    mean = jnp.mean(means, axis=0)
    away = means - mean
    spread = (jnp.sum(spreads, axis=0) + width * jnp.sum(away * away, axis=0)) / (8 * width)
    result = (value - mean[:, None]) * lax.rsqrt(spread + norm_eps)[:, None] * gain_out
    return result.astype(bf16)


def solution(mesh):
    mesh = Mesh(mesh.devices.reshape(8, 8, 4, 2), EVERY)
    return jax.shard_map(
        layer,
        mesh=mesh,
        in_specs=(
            P(FS, TP),
            P(TP),
            P(FS, TP),
            P(TP),
            P(FS, TP),
            P(TP),
            P(FS, TP),
            P(FS, TP),
            P(TP),
        ),
        out_specs=P(FS, TP),
        check_vma=False,
    )
```

```python
import functools

import jax
import jax.numpy as jnp
from jax import lax
from jax.experimental import pallas as pl
from jax.experimental.pallas import tpu as pltpu
from jax.sharding import Mesh, PartitionSpec as P


norm_eps = 1e-05
residual_alpha = 2.0**0.25
FS = ("z", "y")
TP = ("x", "core")
EVERY = FS + TP
bf16 = jnp.bfloat16
f32 = jnp.float32
OFFSETS = (0, 1, -1, 2, -2, 3, -3, 4, 4)
MEBI = 1024 * 1024


def device(z, y, x, core):
    return (((z % 8) * 8 + y % 8) * 4 + x % 4) * 2 + core % 2


PLACES = [(z, y, x) for z in range(8) for y in range(8) for x in range(4)]
FIRST = [[device(z, y, x, 0) for z in range(8)] for y in range(8) for x in range(4)] + [
    [device(z, y, x, 1) for y in range(8)] for z in range(8) for x in range(4)
]
SECOND = [[device(z, y, x, 0) for y in range(8)] for z in range(8) for x in range(4)] + [
    [device(z, y, x, 1) for z in range(8)] for y in range(8) for x in range(4)
]


def around(steps):
    return [
        pair
        for z, y, x in PLACES
        for pair in (
            (device(z, y, x, 0), device(z, y + steps, x, 0)),
            (device(z, y, x, 1), device(z + steps, y, x, 1)),
        )
    ]


def along_x(array, steps):
    pairs = [
        (device(z, y, x, c), device(z, y, x + steps, c)) for z, y, x in PLACES for c in range(2)
    ]
    return lax.ppermute(array, EVERY, pairs)


def from_other_core(array):
    return lax.ppermute(array, "core", [(0, 1), (1, 0)])


def everyone(array, axis):
    count = lax.axis_size(axis)
    return lax.all_to_all(
        jnp.broadcast_to(array[None], (count, *array.shape)), axis, 0, 0, tiled=True
    )


def among(array, groups):
    return lax.all_to_all(
        jnp.broadcast_to(array[None], (8, *array.shape)),
        EVERY,
        0,
        0,
        axis_index_groups=groups,
        tiled=True,
    )


def scatter_sum_tp(keep, send):
    chip = (keep.astype(f32) + from_other_core(send).astype(f32)).astype(bf16)
    four = lax.all_to_all(chip, "x", 0, 0, tiled=True).astype(f32)
    return (four[0] + four[1]) + (four[2] + four[3])


def in_three(gain):
    rest, rows = gain, []
    for _ in range(3):
        rows.append(lax.reduce_precision(rest, 8, 7))
        rest = rest - rows[-1]
    return jnp.stack(rows).astype(bf16)


def gain_of(tok_ref, block, rows, first):
    parts = tok_ref[block, pl.ds(rows, 16), :].astype(f32)
    return parts[first : first + 1] + parts[first + 1 : first + 2] + parts[first + 2 : first + 3]


def columns_of(x, core):
    return pl.ds(pl.multiple_of((2 * x + core) * 256, 256), 256)


def row_at(core, source, j):
    at = jnp.where(core == 0, j * 256 + source * 32, source * 256 + j * 32)
    return pl.ds(pl.multiple_of(at, 32), 32)


def row_statistics(loads, width):
    total = None
    for load in loads:
        s = jnp.sum(load(), axis=1, keepdims=True)
        total = s if total is None else total + s
    mean = total / width
    spread = None
    for load in loads:
        c = load() - mean
        s = jnp.sum(c * c, axis=1, keepdims=True)
        spread = s if spread is None else spread + s
    return mean, lax.rsqrt(spread / width + norm_eps)


def shift_down(value, steps, row):
    return jnp.where(row >= steps, pltpu.roll(value, steps, 0), 0.0)


def mixer_kernel(rows, mine_ref, other_ref, small_ref, scale_ref, keep_ref, send_ref, mixed_ref, w_ref):
    x, core = lax.axis_index("x"), lax.axis_index("core")
    for s in range(8):
        for j in range(8):
            w_ref[row_at(core, s, j), :] = small_ref[s, j]
    step = rows // 3
    for t in range(3):
        part = pl.ds(t * step, step)
        blocks = [(ref, r) for ref in (mine_ref, other_ref) for r in range(4)]
        loads = [lambda ref=ref, r=r: ref[r, part, :].astype(f32) for ref, r in blocks]
        mean, inverse = row_statistics(loads, 2048)
        for (ref, r), load in zip(blocks, loads):
            where = columns_of(lax.rem(x + (4 - r), 4), core if ref is mine_ref else 1 - core)
            mixed = (load() - mean) * inverse * gain_of(ref, r, rows, 0)
            mixed_ref[part, where] = mixed.astype(bf16)
    pool_in = jnp.dot(mixed_ref[...], w_ref[:, :128], preferred_element_type=f32)
    u = pool_in.astype(bf16).astype(f32)
    row = lax.broadcasted_iota(jnp.int32, u.shape, 0)
    two = u + shift_down(u, 1, row)
    four = two + shift_down(two, 2, row)
    eight = four + shift_down(four, 4, row)
    sixteen = eight + shift_down(eight, 8, row)
    total = jnp.where(x == 0, two, jnp.where(x == 1, four, jnp.where(x == 2, eight, sixteen)))
    window = jnp.where(x == 0, 2, jnp.where(x == 1, 4, jnp.where(x == 2, 8, 16)))
    count = jnp.minimum(row + 1, window).astype(f32)
    pooled = ((total / count - u) * scale_ref[...]).astype(bf16)
    for xb in range(4):
        for ref, c in ((keep_ref, core), (send_ref, 1 - core)):
            term = lax.dot_general(
                pooled,
                w_ref[columns_of(xb, c), 128:],
                (((1,), (1,)), ((), ())),
                preferred_element_type=f32,
            )
            ref[xb] = term.astype(bf16)


def ff_kernel(rows, mine_ref, other_ref, mix_ref, mix_other_ref, *refs):
    chunks, (keep_ref, send_ref, own_ref, mid_ref, hid_ref, w_ref, sems) = refs[:9], refs[9:]
    x, core = lax.axis_index("x"), lax.axis_index("core")
    place = jnp.where(core == 0, lax.axis_index("y"), lax.axis_index("z"))
    copies = [[], []]
    for half in range(2):
        where = pl.ds(half * 1024, 1024)
        for k, (chunk, offset) in enumerate(zip(chunks, OFFSETS)):
            source = lax.rem(place + (8 - offset), 8)
            for i in range(8 if k < 7 else 4):
                j = i + 4 if k == 8 else i
                copy = pltpu.make_async_copy(
                    chunk.at[i, :, where],
                    w_ref.at[row_at(core, source, j), where],
                    sems.at[half, min(k, 7), j],
                )
                copy.start()
                copies[half].append(copy)
    step = rows // 3
    for t in range(3):
        part = pl.ds(t * step, step)
        blocks = [
            (tok, mix, c, xb)
            for tok, mix, c in ((mine_ref, mix_ref, core), (other_ref, mix_other_ref, 1 - core))
            for xb in range(4)
        ]

        def total(tok, mix, xb):
            r = lax.rem(x + (4 - xb), 4)
            return residual_alpha * tok[r, part, :].astype(f32) + mix[xb, part, :].astype(f32)

        loads = [functools.partial(total, tok, mix, xb) for tok, mix, _, xb in blocks]
        mean, inverse = row_statistics(loads, 2048)
        for (tok, mix, c, xb), load in zip(blocks, loads):
            gain = gain_of(tok, lax.rem(x + (4 - xb), 4), rows, 3)
            mid_ref[part, columns_of(xb, c)] = ((load() - mean) * inverse * gain).astype(bf16)
    own_ref[...] = mid_ref[:, columns_of(x, core)]
    for copy in copies[0]:
        copy.wait()
    for n in range(4):
        where = slice(n * 256, (n + 1) * 256)
        up = jnp.dot(mid_ref[...], w_ref[:, where], preferred_element_type=f32)
        up = jnp.maximum(up, 0.0)
        hid_ref[:, where] = (up * up).astype(bf16)
    for copy in copies[1]:
        copy.wait()
    for xb in range(4):
        for ref, c in ((keep_ref, core), (send_ref, 1 - core)):
            term = lax.dot_general(
                hid_ref[...],
                w_ref[columns_of(xb, c), 1024:],
                (((1,), (1,)), ((), ())),
                preferred_element_type=f32,
            )
            ref[xb] = term.astype(bf16)


def vmem(count):
    return [pl.BlockSpec(memory_space=pltpu.VMEM)] * count


def mixer(mine, other, small, scale, rows, width, channels):
    block = jax.ShapeDtypeStruct((4, rows, width), bf16)
    return pl.pallas_call(
        functools.partial(mixer_kernel, rows),
        out_shape=(block, block),
        in_specs=vmem(4),
        out_specs=tuple(vmem(2)),
        scratch_shapes=[
            pltpu.VMEM((rows, 8 * width), bf16),
            pltpu.VMEM((8 * width, 2 * channels), bf16),
        ],
        compiler_params=pltpu.CompilerParams(vmem_limit_bytes=24 * MEBI),
        cost_estimate=pl.CostEstimate(flops=4_000_000_000, bytes_accessed=4_000_000, transcendentals=0),
        name="mixer",
    )(mine, other, small, scale)


def feed_forward(mine, other, mix, mix_other, chunks, rows, width):
    block = jax.ShapeDtypeStruct((4, rows, width), bf16)
    return pl.pallas_call(
        functools.partial(ff_kernel, rows),
        out_shape=(block, block, jax.ShapeDtypeStruct((rows, width), bf16)),
        in_specs=vmem(4) + [pl.BlockSpec(memory_space=pl.ANY)] * 9,
        out_specs=tuple(vmem(3)),
        scratch_shapes=[
            pltpu.VMEM((rows, 8 * width), bf16),
            pltpu.VMEM((rows, 1024), bf16),
            pltpu.VMEM((2048, 2048), bf16),
            pltpu.SemaphoreType.DMA((2, 8, 8)),
        ],
        compiler_params=pltpu.CompilerParams(vmem_limit_bytes=30 * MEBI),
        cost_estimate=pl.CostEstimate(flops=8_000_000_000, bytes_accessed=12_000_000, transcendentals=0),
        name="feed_forward",
    )(mine, other, mix, mix_other, *chunks)


def layer(tokens, gain_mixer, w_in, pool_scale, w_pool_out, gain_mid, w_ff1, w_ff2, gain_out):
    rows, width = tokens.shape
    channels = w_in.shape[1]
    packed = jnp.concatenate([w_ff1, w_ff2, w_in, w_pool_out], axis=1)
    first = among(packed, FIRST)
    small = among(first[:, :, 2048:].reshape(256, 2 * channels), SECOND)
    small = small.reshape(8, 8, 32, 2 * channels)
    chunk = first[:, :, :2048]
    chunks = [chunk]
    up, down = chunk, chunk
    for hop in range(4):
        if hop == 3:
            up, down = up[:4], down[4:]
        up = lax.ppermute(up, EVERY, around(1))
        down = lax.ppermute(down, EVERY, around(-1))
        chunks += [up, down]
    extended = jnp.concatenate(
        [tokens, in_three(gain_mixer), in_three(gain_mid), jnp.zeros((10, width), bf16)]
    )
    pieces = [extended]
    for steps in (1, 2, 3):
        pieces.append(along_x(extended, steps))
    mine = jnp.stack(pieces)
    other = from_other_core(mine)
    keep, send = mixer(mine, other, small, pool_scale[None], rows, width, channels)
    mixer_out = scatter_sum_tp(keep, send).astype(bf16)
    mix = everyone(mixer_out, "x")
    mix_other = from_other_core(mix)
    keep, send, middle = feed_forward(mine, other, mix, mix_other, chunks, rows, width)
    ff_out = scatter_sum_tp(keep, send).astype(bf16)
    value = residual_alpha * middle.astype(f32) + ff_out.astype(f32)
    part_mean = jnp.sum(value, axis=1) / width
    center = value - part_mean[:, None]
    part_spread = jnp.sum(center * center, axis=1)
    sums = jnp.concatenate([part_mean, part_spread])[None]
    means, spreads = jnp.split(everyone(sums, TP)[:, 0], 2, axis=1)
    mean = jnp.mean(means, axis=0)
    away = means - mean
    spread = (jnp.sum(spreads, axis=0) + width * jnp.sum(away * away, axis=0)) / (8 * width)
    result = (value - mean[:, None]) * lax.rsqrt(spread + norm_eps)[:, None] * gain_out
    return result.astype(bf16)


def solution(mesh):
    mesh = Mesh(mesh.devices.reshape(8, 8, 4, 2), EVERY)
    return jax.shard_map(
        layer,
        mesh=mesh,
        in_specs=(
            P(FS, TP),
            P(TP),
            P(FS, TP),
            P(TP),
            P(FS, TP),
            P(TP),
            P(FS, TP),
            P(FS, TP),
            P(TP),
        ),
        out_specs=P(FS, TP),
        check_vma=False,
    )
```

```python
import functools

import jax
import jax.numpy as jnp
from jax import lax
from jax.experimental import pallas as pl
from jax.experimental.pallas import tpu as pltpu
from jax.sharding import Mesh, PartitionSpec as P


norm_eps = 1e-05
residual_alpha = 2.0**0.25
FS = ("z", "y")
TP = ("x", "core")
EVERY = FS + TP
bf16 = jnp.bfloat16
f32 = jnp.float32
OFFSETS = (0, -1, 1, -2, 2, -3, 3, -4)
MEBI = 1024 * 1024


def device(z, y, x, core):
    return (((z % 8) * 8 + y % 8) * 4 + x % 4) * 2 + core % 2


PLACES = [(z, y, x) for z in range(8) for y in range(8) for x in range(4)]
FIRST = [[device(z, y, x, 0) for z in range(8)] for y in range(8) for x in range(4)] + [
    [device(z, y, x, 1) for y in range(8)] for z in range(8) for x in range(4)
]
SECOND = [[device(z, y, x, 0) for y in range(8)] for z in range(8) for x in range(4)] + [
    [device(z, y, x, 1) for z in range(8)] for y in range(8) for x in range(4)
]


def around(steps):
    return [
        pair
        for z, y, x in PLACES
        for pair in (
            (device(z, y, x, 0), device(z, y + steps, x, 0)),
            (device(z, y, x, 1), device(z + steps, y, x, 1)),
        )
    ]


def along_x(array, steps):
    pairs = [
        (device(z, y, x, c), device(z, y, x + steps, c)) for z, y, x in PLACES for c in range(2)
    ]
    return lax.ppermute(array, EVERY, pairs)


def from_other_core(array):
    return lax.ppermute(array, "core", [(0, 1), (1, 0)])


def everyone(array, axis):
    count = lax.axis_size(axis)
    return lax.all_to_all(
        jnp.broadcast_to(array[None], (count, *array.shape)), axis, 0, 0, tiled=True
    )


def among(array, groups):
    return lax.all_to_all(
        jnp.broadcast_to(array[None], (8, *array.shape)),
        EVERY,
        0,
        0,
        axis_index_groups=groups,
        tiled=True,
    )


def scatter_sum_tp(keep, send):
    chip = (keep.astype(f32) + from_other_core(send).astype(f32)).astype(bf16)
    four = lax.all_to_all(chip, "x", 0, 0, tiled=True).astype(f32)
    return (four[0] + four[1]) + (four[2] + four[3])


def in_three(gain):
    rest, rows = gain, []
    for _ in range(3):
        rows.append(lax.reduce_precision(rest, 8, 7))
        rest = rest - rows[-1]
    return jnp.stack(rows).astype(bf16)


def gain_of(tok_ref, block, rows, first):
    parts = tok_ref[block, pl.ds(rows, 16), :].astype(f32)
    return parts[first : first + 1] + parts[first + 1 : first + 2] + parts[first + 2 : first + 3]


def columns_of(x, core):
    return pl.ds(pl.multiple_of((2 * x + core) * 256, 256), 256)


def row_at(core, source, j):
    at = jnp.where(core == 0, j * 256 + source * 32, source * 256 + j * 32)
    return pl.ds(pl.multiple_of(at, 32), 32)


def row_statistics(loads, width):
    total = None
    for load in loads:
        s = jnp.sum(load(), axis=1, keepdims=True)
        total = s if total is None else total + s
    mean = total / width
    spread = None
    for load in loads:
        c = load() - mean
        s = jnp.sum(c * c, axis=1, keepdims=True)
        spread = s if spread is None else spread + s
    return mean, lax.rsqrt(spread / width + norm_eps)


def shift_down(value, steps, row):
    return jnp.where(row >= steps, pltpu.roll(value, steps, 0), 0.0)


def mixed_kernel(rows, mine_ref, other_ref, mixed_ref):
    x, core = lax.axis_index("x"), lax.axis_index("core")
    step = rows // 3
    for t in range(3):
        part = pl.ds(t * step, step)
        blocks = [(ref, r) for ref in (mine_ref, other_ref) for r in range(4)]
        loads = [lambda ref=ref, r=r: ref[r, part, :].astype(f32) for ref, r in blocks]
        mean, inverse = row_statistics(loads, 2048)
        for (ref, r), load in zip(blocks, loads):
            where = columns_of(lax.rem(x + (4 - r), 4), core if ref is mine_ref else 1 - core)
            mixed = (load() - mean) * inverse * gain_of(ref, r, rows, 0)
            mixed_ref[part, where] = mixed.astype(bf16)


def mixer_kernel(mixed_ref, small_ref, scale_ref, keep_ref, send_ref, w_ref):
    x, core = lax.axis_index("x"), lax.axis_index("core")
    for s in range(8):
        for j in range(8):
            w_ref[row_at(core, s, j), :] = small_ref[s, j]
    pool_in = jnp.dot(mixed_ref[...], w_ref[:, :128], preferred_element_type=f32)
    u = pool_in.astype(bf16).astype(f32)
    row = lax.broadcasted_iota(jnp.int32, u.shape, 0)
    two = u + shift_down(u, 1, row)
    four = two + shift_down(two, 2, row)
    eight = four + shift_down(four, 4, row)
    sixteen = eight + shift_down(eight, 8, row)
    total = jnp.where(x == 0, two, jnp.where(x == 1, four, jnp.where(x == 2, eight, sixteen)))
    window = jnp.where(x == 0, 2, jnp.where(x == 1, 4, jnp.where(x == 2, 8, 16)))
    count = jnp.minimum(row + 1, window).astype(f32)
    pooled = ((total / count - u) * scale_ref[...]).astype(bf16)
    for xb in range(4):
        for ref, c in ((keep_ref, core), (send_ref, 1 - core)):
            term = lax.dot_general(
                pooled,
                w_ref[columns_of(xb, c), 128:],
                (((1,), (1,)), ((), ())),
                preferred_element_type=f32,
            )
            ref[xb] = term.astype(bf16)


def middle_kernel(rows, mine_ref, other_ref, mix_ref, mix_other_ref, mid_ref, own_ref):
    x, core = lax.axis_index("x"), lax.axis_index("core")
    step = rows // 3
    for t in range(3):
        part = pl.ds(t * step, step)
        blocks = [
            (tok, mix, c, xb)
            for tok, mix, c in ((mine_ref, mix_ref, core), (other_ref, mix_other_ref, 1 - core))
            for xb in range(4)
        ]

        def total(tok, mix, xb):
            r = lax.rem(x + (4 - xb), 4)
            return residual_alpha * tok[r, part, :].astype(f32) + mix[xb, part, :].astype(f32)

        loads = [functools.partial(total, tok, mix, xb) for tok, mix, _, xb in blocks]
        mean, inverse = row_statistics(loads, 2048)
        for (tok, mix, c, xb), load in zip(blocks, loads):
            gain = gain_of(tok, lax.rem(x + (4 - xb), 4), rows, 3)
            mid_ref[part, columns_of(xb, c)] = ((load() - mean) * inverse * gain).astype(bf16)
    own_ref[...] = mid_ref[:, columns_of(x, core)]


def ff_kernel(mid_ref, *refs):
    chunks, (keep_ref, send_ref, hid_ref, w_ref, sems) = refs[:8], refs[8:]
    core = lax.axis_index("core")
    place = jnp.where(core == 0, lax.axis_index("y"), lax.axis_index("z"))
    copies = [[], []]
    for half in range(2):
        where = pl.ds(half * 1024, 1024)
        for k, (chunk, offset) in enumerate(zip(chunks, OFFSETS)):
            source = lax.rem(place + (8 - offset), 8)
            for j in range(8):
                copy = pltpu.make_async_copy(
                    chunk.at[j, :, where],
                    w_ref.at[row_at(core, source, j), where],
                    sems.at[half, k, j],
                )
                copy.start()
                copies[half].append(copy)
    for copy in copies[0]:
        copy.wait()
    for n in range(4):
        where = slice(n * 256, (n + 1) * 256)
        up = jnp.dot(mid_ref[...], w_ref[:, where], preferred_element_type=f32)
        up = jnp.maximum(up, 0.0)
        hid_ref[:, where] = (up * up).astype(bf16)
    for copy in copies[1]:
        copy.wait()
    for xb in range(4):
        for ref, c in ((keep_ref, core), (send_ref, 1 - core)):
            term = lax.dot_general(
                hid_ref[...],
                w_ref[columns_of(xb, c), 1024:],
                (((1,), (1,)), ((), ())),
                preferred_element_type=f32,
            )
            ref[xb] = term.astype(bf16)


def vmem(count):
    return [pl.BlockSpec(memory_space=pltpu.VMEM)] * count


def mixed_of(mine, other, rows, width):
    return pl.pallas_call(
        functools.partial(mixed_kernel, rows),
        out_shape=jax.ShapeDtypeStruct((rows, 8 * width), bf16),
        in_specs=vmem(2),
        out_specs=vmem(1)[0],
        compiler_params=pltpu.CompilerParams(vmem_limit_bytes=16 * MEBI),
        cost_estimate=pl.CostEstimate(flops=2_000_000_000, bytes_accessed=3_000_000, transcendentals=0),
        name="mixed_in",
    )(mine, other)


def mixer(mixed, small, scale, rows, width, channels):
    block = jax.ShapeDtypeStruct((4, rows, width), bf16)
    return pl.pallas_call(
        mixer_kernel,
        out_shape=(block, block),
        in_specs=vmem(3),
        out_specs=tuple(vmem(2)),
        scratch_shapes=[pltpu.VMEM((8 * width, 2 * channels), bf16)],
        compiler_params=pltpu.CompilerParams(vmem_limit_bytes=24 * MEBI),
        cost_estimate=pl.CostEstimate(flops=2_000_000_000, bytes_accessed=4_000_000, transcendentals=0),
        name="mixer",
    )(mixed, small, scale)


def middle_of(mine, other, mix, mix_other, rows, width):
    return pl.pallas_call(
        functools.partial(middle_kernel, rows),
        out_shape=(
            jax.ShapeDtypeStruct((rows, 8 * width), bf16),
            jax.ShapeDtypeStruct((rows, width), bf16),
        ),
        in_specs=vmem(4),
        out_specs=tuple(vmem(2)),
        compiler_params=pltpu.CompilerParams(vmem_limit_bytes=16 * MEBI),
        cost_estimate=pl.CostEstimate(flops=2_000_000_000, bytes_accessed=5_000_000, transcendentals=0),
        name="middle",
    )(mine, other, mix, mix_other)


def feed_forward(full, chunks, rows, width):
    block = jax.ShapeDtypeStruct((4, rows, width), bf16)
    return pl.pallas_call(
        ff_kernel,
        out_shape=(block, block),
        in_specs=vmem(1) + [pl.BlockSpec(memory_space=pl.ANY)] * 8,
        out_specs=tuple(vmem(2)),
        scratch_shapes=[
            pltpu.VMEM((rows, 1024), bf16),
            pltpu.VMEM((2048, 2048), bf16),
            pltpu.SemaphoreType.DMA((2, 8, 8)),
        ],
        compiler_params=pltpu.CompilerParams(vmem_limit_bytes=30 * MEBI),
        cost_estimate=pl.CostEstimate(flops=6_000_000_000, bytes_accessed=12_000_000, transcendentals=0),
        name="feed_forward",
    )(full, *chunks)


def layer(tokens, gain_mixer, w_in, pool_scale, w_pool_out, gain_mid, w_ff1, w_ff2, gain_out):
    rows, width = tokens.shape
    channels = w_in.shape[1]
    packed = jnp.concatenate([w_ff1, w_ff2, w_in, w_pool_out], axis=1)
    first = among(packed, FIRST)
    small = among(first[:, :, 2048:].reshape(256, 2 * channels), SECOND)
    small = small.reshape(8, 8, 32, 2 * channels)
    chunk = first[:, :, :2048]
    chunks = [chunk]
    up, down = chunk, chunk
    for hop in range(4):
        down = lax.ppermute(down, EVERY, around(-1))
        chunks.append(down)
        if hop < 3:
            up = lax.ppermute(up, EVERY, around(1))
            chunks.append(up)
    extended = jnp.concatenate(
        [tokens, in_three(gain_mixer), in_three(gain_mid), jnp.zeros((10, width), bf16)]
    )
    pieces = [extended]
    for steps in (1, 2, 3):
        pieces.append(along_x(extended, steps))
    mine = jnp.stack(pieces)
    other = from_other_core(mine)
    mixed = mixed_of(mine, other, rows, width)
    keep, send = mixer(mixed, small, pool_scale[None], rows, width, channels)
    mixer_out = scatter_sum_tp(keep, send).astype(bf16)
    mix = everyone(mixer_out, "x")
    mix_other = from_other_core(mix)
    full, middle = middle_of(mine, other, mix, mix_other, rows, width)
    keep, send = feed_forward(full, chunks, rows, width)
    ff_out = scatter_sum_tp(keep, send).astype(bf16)
    value = residual_alpha * middle.astype(f32) + ff_out.astype(f32)
    part_mean = jnp.sum(value, axis=1) / width
    center = value - part_mean[:, None]
    part_spread = jnp.sum(center * center, axis=1)
    sums = jnp.concatenate([part_mean, part_spread])[None]
    means, spreads = jnp.split(everyone(sums, TP)[:, 0], 2, axis=1)
    mean = jnp.mean(means, axis=0)
    away = means - mean
    spread = (jnp.sum(spreads, axis=0) + width * jnp.sum(away * away, axis=0)) / (8 * width)
    result = (value - mean[:, None]) * lax.rsqrt(spread + norm_eps)[:, None] * gain_out
    return result.astype(bf16)


def solution(mesh):
    mesh = Mesh(mesh.devices.reshape(8, 8, 4, 2), EVERY)
    return jax.shard_map(
        layer,
        mesh=mesh,
        in_specs=(
            P(FS, TP),
            P(TP),
            P(FS, TP),
            P(TP),
            P(FS, TP),
            P(TP),
            P(FS, TP),
            P(FS, TP),
            P(TP),
        ),
        out_specs=P(FS, TP),
        check_vma=False,
    )
```

```python
import functools

import jax
import jax.numpy as jnp
from jax import lax
from jax.experimental import pallas as pl
from jax.experimental.pallas import tpu as pltpu
from jax.sharding import Mesh, PartitionSpec as P


norm_eps = 1e-05
residual_alpha = 2.0**0.25
FS = ("z", "y")
TP = ("x", "core")
EVERY = FS + TP
bf16 = jnp.bfloat16
f32 = jnp.float32
OFFSETS = (0, -1, 1, -2, 2, -3, 3, -4)
MEBI = 1024 * 1024


def device(z, y, x, core):
    return (((z % 8) * 8 + y % 8) * 4 + x % 4) * 2 + core % 2


PLACES = [(z, y, x) for z in range(8) for y in range(8) for x in range(4)]
FIRST = [[device(z, y, x, 0) for z in range(8)] for y in range(8) for x in range(4)] + [
    [device(z, y, x, 1) for y in range(8)] for z in range(8) for x in range(4)
]
SECOND = [[device(z, y, x, 0) for y in range(8)] for z in range(8) for x in range(4)] + [
    [device(z, y, x, 1) for z in range(8)] for y in range(8) for x in range(4)
]


def around(steps):
    return [
        pair
        for z, y, x in PLACES
        for pair in (
            (device(z, y, x, 0), device(z, y + steps, x, 0)),
            (device(z, y, x, 1), device(z + steps, y, x, 1)),
        )
    ]


def along_x(array, steps):
    pairs = [
        (device(z, y, x, c), device(z, y, x + steps, c)) for z, y, x in PLACES for c in range(2)
    ]
    return lax.ppermute(array, EVERY, pairs)


def from_other_core(array):
    return lax.ppermute(array, "core", [(0, 1), (1, 0)])


def everyone(array, axis):
    count = lax.axis_size(axis)
    return lax.all_to_all(
        jnp.broadcast_to(array[None], (count, *array.shape)), axis, 0, 0, tiled=True
    )


def among(array, groups):
    return lax.all_to_all(
        jnp.broadcast_to(array[None], (8, *array.shape)),
        EVERY,
        0,
        0,
        axis_index_groups=groups,
        tiled=True,
    )


def scatter_sum_tp(keep, send):
    chip = (keep.astype(f32) + from_other_core(send).astype(f32)).astype(bf16)
    four = lax.all_to_all(chip, "x", 0, 0, tiled=True).astype(f32)
    return (four[0] + four[1]) + (four[2] + four[3])


def in_three(gain):
    rest, rows = gain, []
    for _ in range(3):
        rows.append(lax.reduce_precision(rest, 8, 7))
        rest = rest - rows[-1]
    return jnp.stack(rows).astype(bf16)


def gain_of(tok_ref, block, rows, first):
    parts = tok_ref[block, pl.ds(rows, 16), :].astype(f32)
    return parts[first : first + 1] + parts[first + 1 : first + 2] + parts[first + 2 : first + 3]


def columns_of(x, core):
    return pl.ds(pl.multiple_of((2 * x + core) * 256, 256), 256)


def row_at(core, source, j):
    at = jnp.where(core == 0, j * 256 + source * 32, source * 256 + j * 32)
    return pl.ds(pl.multiple_of(at, 32), 32)


def row_statistics(loads, width):
    total = None
    for load in loads:
        s = jnp.sum(load(), axis=1, keepdims=True)
        total = s if total is None else total + s
    mean = total / width
    spread = None
    for load in loads:
        c = load() - mean
        s = jnp.sum(c * c, axis=1, keepdims=True)
        spread = s if spread is None else spread + s
    return mean, lax.rsqrt(spread / width + norm_eps)


def shift_down(value, steps, row):
    return jnp.where(row >= steps, pltpu.roll(value, steps, 0), 0.0)


def mixer_kernel(rows, mine_ref, other_ref, small_ref, scale_ref, keep_ref, send_ref, mixed_ref, w_ref):
    x, core = lax.axis_index("x"), lax.axis_index("core")
    for s in range(8):
        for j in range(8):
            w_ref[row_at(core, s, j), :] = small_ref[s, j]
    step = rows // 3
    for t in range(3):
        part = pl.ds(t * step, step)
        blocks = [(ref, r) for ref in (mine_ref, other_ref) for r in range(4)]
        loads = [lambda ref=ref, r=r: ref[r, part, :].astype(f32) for ref, r in blocks]
        mean, inverse = row_statistics(loads, 2048)
        for (ref, r), load in zip(blocks, loads):
            where = columns_of(lax.rem(x + (4 - r), 4), core if ref is mine_ref else 1 - core)
            mixed = (load() - mean) * inverse * gain_of(ref, r, rows, 0)
            mixed_ref[part, where] = mixed.astype(bf16)
    pool_in = jnp.dot(mixed_ref[...], w_ref[:, :128], preferred_element_type=f32)
    u = pool_in.astype(bf16).astype(f32)
    row = lax.broadcasted_iota(jnp.int32, u.shape, 0)
    two = u + shift_down(u, 1, row)
    four = two + shift_down(two, 2, row)
    eight = four + shift_down(four, 4, row)
    sixteen = eight + shift_down(eight, 8, row)
    total = jnp.where(x == 0, two, jnp.where(x == 1, four, jnp.where(x == 2, eight, sixteen)))
    window = jnp.where(x == 0, 2, jnp.where(x == 1, 4, jnp.where(x == 2, 8, 16)))
    count = jnp.minimum(row + 1, window).astype(f32)
    pooled = ((total / count - u) * scale_ref[...]).astype(bf16)
    for xb in range(4):
        for ref, c in ((keep_ref, core), (send_ref, 1 - core)):
            term = lax.dot_general(
                pooled,
                w_ref[columns_of(xb, c), 128:],
                (((1,), (1,)), ((), ())),
                preferred_element_type=f32,
            )
            ref[xb] = term.astype(bf16)


def middle_kernel(rows, mine_ref, other_ref, mix_ref, mix_other_ref, mid_ref, own_ref):
    x, core = lax.axis_index("x"), lax.axis_index("core")
    step = rows // 3
    for t in range(3):
        part = pl.ds(t * step, step)
        blocks = [
            (tok, mix, c, xb)
            for tok, mix, c in ((mine_ref, mix_ref, core), (other_ref, mix_other_ref, 1 - core))
            for xb in range(4)
        ]

        def total(tok, mix, xb):
            r = lax.rem(x + (4 - xb), 4)
            return residual_alpha * tok[r, part, :].astype(f32) + mix[xb, part, :].astype(f32)

        loads = [functools.partial(total, tok, mix, xb) for tok, mix, _, xb in blocks]
        mean, inverse = row_statistics(loads, 2048)
        for (tok, mix, c, xb), load in zip(blocks, loads):
            gain = gain_of(tok, lax.rem(x + (4 - xb), 4), rows, 3)
            mid_ref[part, columns_of(xb, c)] = ((load() - mean) * inverse * gain).astype(bf16)
    own_ref[...] = mid_ref[:, columns_of(x, core)]


def ff_kernel(mid_ref, *refs):
    chunks, (keep_ref, send_ref, hid_ref, w_ref, sems) = refs[:8], refs[8:]
    core = lax.axis_index("core")
    place = jnp.where(core == 0, lax.axis_index("y"), lax.axis_index("z"))
    copies = [[], []]
    for half in range(2):
        where = pl.ds(half * 1024, 1024)
        for k, (chunk, offset) in enumerate(zip(chunks, OFFSETS)):
            source = lax.rem(place + (8 - offset), 8)
            for j in range(8):
                copy = pltpu.make_async_copy(
                    chunk.at[j, :, where],
                    w_ref.at[row_at(core, source, j), where],
                    sems.at[half, k, j],
                )
                copy.start()
                copies[half].append(copy)
    for copy in copies[0]:
        copy.wait()
    for n in range(4):
        where = slice(n * 256, (n + 1) * 256)
        up = jnp.dot(mid_ref[...], w_ref[:, where], preferred_element_type=f32)
        up = jnp.maximum(up, 0.0)
        hid_ref[:, where] = (up * up).astype(bf16)
    for copy in copies[1]:
        copy.wait()
    for xb in range(4):
        for ref, c in ((keep_ref, core), (send_ref, 1 - core)):
            term = lax.dot_general(
                hid_ref[...],
                w_ref[columns_of(xb, c), 1024:],
                (((1,), (1,)), ((), ())),
                preferred_element_type=f32,
            )
            ref[xb] = term.astype(bf16)


def vmem(count):
    return [pl.BlockSpec(memory_space=pltpu.VMEM)] * count


def mixer(mine, other, small, scale, rows, width, channels):
    block = jax.ShapeDtypeStruct((4, rows, width), bf16)
    return pl.pallas_call(
        functools.partial(mixer_kernel, rows),
        out_shape=(block, block),
        in_specs=vmem(4),
        out_specs=tuple(vmem(2)),
        scratch_shapes=[
            pltpu.VMEM((rows, 8 * width), bf16),
            pltpu.VMEM((8 * width, 2 * channels), bf16),
        ],
        compiler_params=pltpu.CompilerParams(vmem_limit_bytes=24 * MEBI),
        cost_estimate=pl.CostEstimate(flops=4_000_000_000, bytes_accessed=4_000_000, transcendentals=0),
        name="mixer",
    )(mine, other, small, scale)


def middle_of(mine, other, mix, mix_other, rows, width):
    return pl.pallas_call(
        functools.partial(middle_kernel, rows),
        out_shape=(
            jax.ShapeDtypeStruct((rows, 8 * width), bf16),
            jax.ShapeDtypeStruct((rows, width), bf16),
        ),
        in_specs=vmem(4),
        out_specs=tuple(vmem(2)),
        compiler_params=pltpu.CompilerParams(vmem_limit_bytes=16 * MEBI),
        cost_estimate=pl.CostEstimate(flops=2_000_000_000, bytes_accessed=5_000_000, transcendentals=0),
        name="middle",
    )(mine, other, mix, mix_other)


def feed_forward(full, chunks, rows, width):
    block = jax.ShapeDtypeStruct((4, rows, width), bf16)
    return pl.pallas_call(
        ff_kernel,
        out_shape=(block, block),
        in_specs=vmem(1) + [pl.BlockSpec(memory_space=pl.ANY)] * 8,
        out_specs=tuple(vmem(2)),
        scratch_shapes=[
            pltpu.VMEM((rows, 1024), bf16),
            pltpu.VMEM((2048, 2048), bf16),
            pltpu.SemaphoreType.DMA((2, 8, 8)),
        ],
        compiler_params=pltpu.CompilerParams(vmem_limit_bytes=30 * MEBI),
        cost_estimate=pl.CostEstimate(flops=6_000_000_000, bytes_accessed=12_000_000, transcendentals=0),
        name="feed_forward",
    )(full, *chunks)


def layer(tokens, gain_mixer, w_in, pool_scale, w_pool_out, gain_mid, w_ff1, w_ff2, gain_out):
    rows, width = tokens.shape
    channels = w_in.shape[1]
    packed = jnp.concatenate([w_ff1, w_ff2, w_in, w_pool_out], axis=1)
    first = among(packed, FIRST)
    small = among(first[:, :, 2048:].reshape(256, 2 * channels), SECOND)
    small = small.reshape(8, 8, 32, 2 * channels)
    chunk = first[:, :, :2048]
    chunks = [chunk]
    up, down = chunk, chunk
    for hop in range(4):
        down = lax.ppermute(down, EVERY, around(-1))
        chunks.append(down)
        if hop < 3:
            up = lax.ppermute(up, EVERY, around(1))
            chunks.append(up)
    extended = jnp.concatenate(
        [tokens, in_three(gain_mixer), in_three(gain_mid), jnp.zeros((10, width), bf16)]
    )
    pieces = [extended]
    for steps in (1, 2, 3):
        pieces.append(along_x(extended, steps))
    mine = jnp.stack(pieces)
    other = from_other_core(mine)
    keep, send = mixer(mine, other, small, pool_scale[None], rows, width, channels)
    mixer_out = scatter_sum_tp(keep, send).astype(bf16)
    mix = everyone(mixer_out, "x")
    mix_other = from_other_core(mix)
    full, middle = middle_of(mine, other, mix, mix_other, rows, width)
    keep, send = feed_forward(full, chunks, rows, width)
    ff_out = scatter_sum_tp(keep, send).astype(bf16)
    value = residual_alpha * middle.astype(f32) + ff_out.astype(f32)
    part_mean = jnp.sum(value, axis=1) / width
    center = value - part_mean[:, None]
    part_spread = jnp.sum(center * center, axis=1)
    sums = jnp.concatenate([part_mean, part_spread])[None]
    means, spreads = jnp.split(everyone(sums, TP)[:, 0], 2, axis=1)
    mean = jnp.mean(means, axis=0)
    away = means - mean
    spread = (jnp.sum(spreads, axis=0) + width * jnp.sum(away * away, axis=0)) / (8 * width)
    result = (value - mean[:, None]) * lax.rsqrt(spread + norm_eps)[:, None] * gain_out
    return result.astype(bf16)


def solution(mesh):
    mesh = Mesh(mesh.devices.reshape(8, 8, 4, 2), EVERY)
    return jax.shard_map(
        layer,
        mesh=mesh,
        in_specs=(
            P(FS, TP),
            P(TP),
            P(FS, TP),
            P(TP),
            P(FS, TP),
            P(TP),
            P(FS, TP),
            P(FS, TP),
            P(TP),
        ),
        out_specs=P(FS, TP),
        check_vma=False,
    )
```

```python
import functools

import jax
import jax.numpy as jnp
from jax import lax
from jax.experimental import pallas as pl
from jax.experimental.pallas import tpu as pltpu
from jax.sharding import Mesh, PartitionSpec as P


norm_eps = 1e-05
residual_alpha = 2.0**0.25
FS = ("z", "y")
TP = ("x", "core")
EVERY = FS + TP
bf16 = jnp.bfloat16
f32 = jnp.float32
OFFSETS = (0, -1, 1, -2, 2, -3, 3, -4)
MEBI = 1024 * 1024


def device(z, y, x, core):
    return (((z % 8) * 8 + y % 8) * 4 + x % 4) * 2 + core % 2


PLACES = [(z, y, x) for z in range(8) for y in range(8) for x in range(4)]
FIRST = [[device(z, y, x, 0) for z in range(8)] for y in range(8) for x in range(4)] + [
    [device(z, y, x, 1) for y in range(8)] for z in range(8) for x in range(4)
]
SECOND = [[device(z, y, x, 0) for y in range(8)] for z in range(8) for x in range(4)] + [
    [device(z, y, x, 1) for z in range(8)] for y in range(8) for x in range(4)
]


def around(steps):
    return [
        pair
        for z, y, x in PLACES
        for pair in (
            (device(z, y, x, 0), device(z, y + steps, x, 0)),
            (device(z, y, x, 1), device(z + steps, y, x, 1)),
        )
    ]


def along_x(array, steps):
    pairs = [
        (device(z, y, x, c), device(z, y, x + steps, c)) for z, y, x in PLACES for c in range(2)
    ]
    return lax.ppermute(array, EVERY, pairs)


def from_other_core(array):
    return lax.ppermute(array, "core", [(0, 1), (1, 0)])


def everyone(array, axis):
    count = lax.axis_size(axis)
    return lax.all_to_all(
        jnp.broadcast_to(array[None], (count, *array.shape)), axis, 0, 0, tiled=True
    )


def eight(array):
    return jnp.broadcast_to(array[None], (8, *array.shape))


def exchanged(blocks, groups):
    return lax.all_to_all(blocks, EVERY, 0, 0, axis_index_groups=groups, tiled=True)


def scatter_sum_tp(keep, send):
    chip = (keep.astype(f32) + from_other_core(send).astype(f32)).astype(bf16)
    four = lax.all_to_all(chip, "x", 0, 0, tiled=True).astype(f32)
    return (four[0] + four[1]) + (four[2] + four[3])


def in_three(gain):
    rest, rows = gain, []
    for _ in range(3):
        rows.append(lax.reduce_precision(rest, 8, 7))
        rest = rest - rows[-1]
    return jnp.stack(rows).astype(bf16)


def gain_of(tok_ref, block, rows, first):
    parts = tok_ref[block, pl.ds(rows, 16), :].astype(f32)
    return parts[first : first + 1] + parts[first + 1 : first + 2] + parts[first + 2 : first + 3]


def columns_of(x, core):
    return pl.ds(pl.multiple_of((2 * x + core) * 256, 256), 256)


def row_at(core, source, j):
    at = jnp.where(core == 0, j * 256 + source * 32, source * 256 + j * 32)
    return pl.ds(pl.multiple_of(at, 32), 32)


def row_statistics(loads, width):
    total = None
    for load in loads:
        s = jnp.sum(load(), axis=1, keepdims=True)
        total = s if total is None else total + s
    mean = total / width
    spread = None
    for load in loads:
        c = load() - mean
        s = jnp.sum(c * c, axis=1, keepdims=True)
        spread = s if spread is None else spread + s
    return mean, lax.rsqrt(spread / width + norm_eps)


def shift_down(value, steps, row):
    return jnp.where(row >= steps, pltpu.roll(value, steps, 0), 0.0)


def mixer_kernel(rows, mine_ref, other_ref, small_ref, scale_ref, keep_ref, send_ref, mixed_ref, w_ref):
    x, core = lax.axis_index("x"), lax.axis_index("core")
    for s in range(8):
        for j in range(8):
            w_ref[row_at(core, s, j), :] = small_ref[s, j]
    step = rows // 3
    for t in range(3):
        part = pl.ds(t * step, step)
        blocks = [(ref, r) for ref in (mine_ref, other_ref) for r in range(4)]
        loads = [lambda ref=ref, r=r: ref[r, part, :].astype(f32) for ref, r in blocks]
        mean, inverse = row_statistics(loads, 2048)
        for (ref, r), load in zip(blocks, loads):
            where = columns_of(lax.rem(x + (4 - r), 4), core if ref is mine_ref else 1 - core)
            mixed = (load() - mean) * inverse * gain_of(ref, r, rows, 0)
            mixed_ref[part, where] = mixed.astype(bf16)
    pool_in = jnp.dot(mixed_ref[...], w_ref[:, :128], preferred_element_type=f32)
    u = pool_in.astype(bf16).astype(f32)
    row = lax.broadcasted_iota(jnp.int32, u.shape, 0)
    two = u + shift_down(u, 1, row)
    four = two + shift_down(two, 2, row)
    eight = four + shift_down(four, 4, row)
    sixteen = eight + shift_down(eight, 8, row)
    total = jnp.where(x == 0, two, jnp.where(x == 1, four, jnp.where(x == 2, eight, sixteen)))
    window = jnp.where(x == 0, 2, jnp.where(x == 1, 4, jnp.where(x == 2, 8, 16)))
    count = jnp.minimum(row + 1, window).astype(f32)
    pooled = ((total / count - u) * scale_ref[...]).astype(bf16)
    for xb in range(4):
        for ref, c in ((keep_ref, core), (send_ref, 1 - core)):
            term = lax.dot_general(
                pooled,
                w_ref[columns_of(xb, c), 128:],
                (((1,), (1,)), ((), ())),
                preferred_element_type=f32,
            )
            ref[xb] = term.astype(bf16)


def middle_kernel(rows, mine_ref, other_ref, mix_ref, mix_other_ref, mid_ref, own_ref):
    x, core = lax.axis_index("x"), lax.axis_index("core")
    step = rows // 3
    for t in range(3):
        part = pl.ds(t * step, step)
        blocks = [
            (tok, mix, c, xb)
            for tok, mix, c in ((mine_ref, mix_ref, core), (other_ref, mix_other_ref, 1 - core))
            for xb in range(4)
        ]

        def total(tok, mix, xb):
            r = lax.rem(x + (4 - xb), 4)
            return residual_alpha * tok[r, part, :].astype(f32) + mix[xb, part, :].astype(f32)

        loads = [functools.partial(total, tok, mix, xb) for tok, mix, _, xb in blocks]
        mean, inverse = row_statistics(loads, 2048)
        for (tok, mix, c, xb), load in zip(blocks, loads):
            gain = gain_of(tok, lax.rem(x + (4 - xb), 4), rows, 3)
            mid_ref[part, columns_of(xb, c)] = ((load() - mean) * inverse * gain).astype(bf16)
    own_ref[...] = mid_ref[:, columns_of(x, core)]


def ff_kernel(mid_ref, *refs):
    chunks, (keep_ref, send_ref, hid_ref, w_ref, sems) = refs[:8], refs[8:]
    core = lax.axis_index("core")
    place = jnp.where(core == 0, lax.axis_index("y"), lax.axis_index("z"))
    copies = [[], []]
    for half in range(2):
        where = pl.ds(half * 1024, 1024)
        for k, (chunk, offset) in enumerate(zip(chunks, OFFSETS)):
            source = lax.rem(place + (8 - offset), 8)
            for j in range(8):
                copy = pltpu.make_async_copy(
                    chunk.at[j, :, where],
                    w_ref.at[row_at(core, source, j), where],
                    sems.at[half, k, j],
                )
                copy.start()
                copies[half].append(copy)
    for copy in copies[0]:
        copy.wait()
    for n in range(4):
        where = slice(n * 256, (n + 1) * 256)
        up = jnp.dot(mid_ref[...], w_ref[:, where], preferred_element_type=f32)
        up = jnp.maximum(up, 0.0)
        hid_ref[:, where] = (up * up).astype(bf16)
    for copy in copies[1]:
        copy.wait()
    for xb in range(4):
        for ref, c in ((keep_ref, core), (send_ref, 1 - core)):
            term = lax.dot_general(
                hid_ref[...],
                w_ref[columns_of(xb, c), 1024:],
                (((1,), (1,)), ((), ())),
                preferred_element_type=f32,
            )
            ref[xb] = term.astype(bf16)


def vmem(count):
    return [pl.BlockSpec(memory_space=pltpu.VMEM)] * count


def split_kernel(first_ref, chunk_ref, blocks_ref, small_ref, sems):
    small = pltpu.make_async_copy(first_ref.at[:, :, pl.ds(2048, 256)], small_ref, sems.at[0])
    chunk = pltpu.make_async_copy(first_ref.at[:, :, pl.ds(0, 2048)], chunk_ref, sems.at[1])
    small.start()
    chunk.start()
    small.wait()
    rows = small_ref[...].reshape(256, 256)
    for i in range(8):
        blocks_ref[i] = rows
    chunk.wait()


def split(first):
    return pl.pallas_call(
        split_kernel,
        out_shape=(
            jax.ShapeDtypeStruct((8, 32, 2048), bf16),
            jax.ShapeDtypeStruct((8, 256, 256), bf16),
        ),
        in_specs=[pl.BlockSpec(memory_space=pl.ANY)],
        out_specs=tuple(vmem(2)),
        scratch_shapes=[pltpu.VMEM((8, 32, 256), bf16), pltpu.SemaphoreType.DMA((2,))],
        compiler_params=pltpu.CompilerParams(vmem_limit_bytes=8 * MEBI),
        cost_estimate=pl.CostEstimate(flops=1_000_000, bytes_accessed=3_000_000, transcendentals=0),
        name="split",
    )(first)


def mixer(mine, other, small, scale, rows, width, channels):
    block = jax.ShapeDtypeStruct((4, rows, width), bf16)
    return pl.pallas_call(
        functools.partial(mixer_kernel, rows),
        out_shape=(block, block),
        in_specs=vmem(4),
        out_specs=tuple(vmem(2)),
        scratch_shapes=[
            pltpu.VMEM((rows, 8 * width), bf16),
            pltpu.VMEM((8 * width, 2 * channels), bf16),
        ],
        compiler_params=pltpu.CompilerParams(vmem_limit_bytes=24 * MEBI),
        cost_estimate=pl.CostEstimate(flops=4_000_000_000, bytes_accessed=4_000_000, transcendentals=0),
        name="mixer",
    )(mine, other, small, scale)


def middle_of(mine, other, mix, mix_other, rows, width):
    return pl.pallas_call(
        functools.partial(middle_kernel, rows),
        out_shape=(
            jax.ShapeDtypeStruct((rows, 8 * width), bf16),
            jax.ShapeDtypeStruct((rows, width), bf16),
        ),
        in_specs=vmem(4),
        out_specs=tuple(vmem(2)),
        compiler_params=pltpu.CompilerParams(vmem_limit_bytes=16 * MEBI),
        cost_estimate=pl.CostEstimate(flops=2_000_000_000, bytes_accessed=5_000_000, transcendentals=0),
        name="middle",
    )(mine, other, mix, mix_other)


def feed_forward(full, chunks, rows, width):
    block = jax.ShapeDtypeStruct((4, rows, width), bf16)
    return pl.pallas_call(
        ff_kernel,
        out_shape=(block, block),
        in_specs=vmem(1) + [pl.BlockSpec(memory_space=pl.ANY)] * 8,
        out_specs=tuple(vmem(2)),
        scratch_shapes=[
            pltpu.VMEM((rows, 1024), bf16),
            pltpu.VMEM((2048, 2048), bf16),
            pltpu.SemaphoreType.DMA((2, 8, 8)),
        ],
        compiler_params=pltpu.CompilerParams(vmem_limit_bytes=30 * MEBI),
        cost_estimate=pl.CostEstimate(flops=6_000_000_000, bytes_accessed=12_000_000, transcendentals=0),
        name="feed_forward",
    )(full, *chunks)


def layer(tokens, gain_mixer, w_in, pool_scale, w_pool_out, gain_mid, w_ff1, w_ff2, gain_out):
    rows, width = tokens.shape
    channels = w_in.shape[1]
    packed = jnp.concatenate([w_ff1, w_ff2, w_in, w_pool_out], axis=1)
    first = exchanged(eight(packed), FIRST)
    chunk, blocks = split(first)
    small = exchanged(blocks, SECOND)
    small = small.reshape(8, 8, 32, 2 * channels)
    chunks = [chunk]
    up, down = chunk, chunk
    for hop in range(4):
        down = lax.ppermute(down, EVERY, around(-1))
        chunks.append(down)
        if hop < 3:
            up = lax.ppermute(up, EVERY, around(1))
            chunks.append(up)
    extended = jnp.concatenate(
        [tokens, in_three(gain_mixer), in_three(gain_mid), jnp.zeros((10, width), bf16)]
    )
    pieces = [extended]
    for steps in (1, 2, 3):
        pieces.append(along_x(extended, steps))
    mine = jnp.stack(pieces)
    other = from_other_core(mine)
    keep, send = mixer(mine, other, small, pool_scale[None], rows, width, channels)
    mixer_out = scatter_sum_tp(keep, send).astype(bf16)
    mix = everyone(mixer_out, "x")
    mix_other = from_other_core(mix)
    full, middle = middle_of(mine, other, mix, mix_other, rows, width)
    keep, send = feed_forward(full, chunks, rows, width)
    ff_out = scatter_sum_tp(keep, send).astype(bf16)
    value = residual_alpha * middle.astype(f32) + ff_out.astype(f32)
    part_mean = jnp.sum(value, axis=1) / width
    center = value - part_mean[:, None]
    part_spread = jnp.sum(center * center, axis=1)
    sums = jnp.concatenate([part_mean, part_spread])[None]
    means, spreads = jnp.split(everyone(sums, TP)[:, 0], 2, axis=1)
    mean = jnp.mean(means, axis=0)
    away = means - mean
    spread = (jnp.sum(spreads, axis=0) + width * jnp.sum(away * away, axis=0)) / (8 * width)
    result = (value - mean[:, None]) * lax.rsqrt(spread + norm_eps)[:, None] * gain_out
    return result.astype(bf16)


def solution(mesh):
    mesh = Mesh(mesh.devices.reshape(8, 8, 4, 2), EVERY)
    return jax.shard_map(
        layer,
        mesh=mesh,
        in_specs=(
            P(FS, TP),
            P(TP),
            P(FS, TP),
            P(TP),
            P(FS, TP),
            P(TP),
            P(FS, TP),
            P(FS, TP),
            P(TP),
        ),
        out_specs=P(FS, TP),
        check_vma=False,
    )
```

```python
import functools

import jax
import jax.numpy as jnp
from jax import lax
from jax.experimental import pallas as pl
from jax.experimental.pallas import tpu as pltpu
from jax.sharding import Mesh, PartitionSpec as P


norm_eps = 1e-05
residual_alpha = 2.0**0.25
FS = ("z", "y")
TP = ("x", "core")
EVERY = FS + TP
bf16 = jnp.bfloat16
f32 = jnp.float32
OFFSETS = (0, -1, 1, -2, 2, -3, 3, -4)
MEBI = 1024 * 1024


def device(z, y, x, core):
    return (((z % 8) * 8 + y % 8) * 4 + x % 4) * 2 + core % 2


PLACES = [(z, y, x) for z in range(8) for y in range(8) for x in range(4)]
FIRST = [[device(z, y, x, 0) for z in range(8)] for y in range(8) for x in range(4)] + [
    [device(z, y, x, 1) for y in range(8)] for z in range(8) for x in range(4)
]
SECOND = [[device(z, y, x, 0) for y in range(8)] for z in range(8) for x in range(4)] + [
    [device(z, y, x, 1) for z in range(8)] for y in range(8) for x in range(4)
]


def around(steps):
    return [
        pair
        for z, y, x in PLACES
        for pair in (
            (device(z, y, x, 0), device(z, y + steps, x, 0)),
            (device(z, y, x, 1), device(z + steps, y, x, 1)),
        )
    ]


def along_x(array, steps):
    pairs = [
        (device(z, y, x, c), device(z, y, x + steps, c)) for z, y, x in PLACES for c in range(2)
    ]
    return lax.ppermute(array, EVERY, pairs)


def from_other_core(array):
    return lax.ppermute(array, "core", [(0, 1), (1, 0)])


def everyone(array, axis):
    count = lax.axis_size(axis)
    return lax.all_to_all(
        jnp.broadcast_to(array[None], (count, *array.shape)), axis, 0, 0, tiled=True
    )


def exchanged(blocks, groups):
    return lax.all_to_all(blocks, EVERY, 0, 0, axis_index_groups=groups, tiled=True)


def scatter_sum_tp(keep, send):
    chip = (keep.astype(f32) + from_other_core(send).astype(f32)).astype(bf16)
    four = lax.all_to_all(chip, "x", 0, 0, tiled=True).astype(f32)
    return (four[0] + four[1]) + (four[2] + four[3])


def in_three(gain):
    rest, rows = gain, []
    for _ in range(3):
        rows.append(lax.reduce_precision(rest, 8, 7))
        rest = rest - rows[-1]
    return jnp.stack(rows).astype(bf16)


def gain_of(tok_ref, block, rows, first):
    parts = tok_ref[block, pl.ds(rows, 16), :].astype(f32)
    return parts[first : first + 1] + parts[first + 1 : first + 2] + parts[first + 2 : first + 3]


def columns_of(x, core):
    return pl.ds(pl.multiple_of((2 * x + core) * 256, 256), 256)


def row_at(core, source, j):
    at = jnp.where(core == 0, j * 256 + source * 32, source * 256 + j * 32)
    return pl.ds(pl.multiple_of(at, 32), 32)


def row_statistics(loads, width):
    total = None
    for load in loads:
        s = jnp.sum(load(), axis=1, keepdims=True)
        total = s if total is None else total + s
    mean = total / width
    spread = None
    for load in loads:
        c = load() - mean
        s = jnp.sum(c * c, axis=1, keepdims=True)
        spread = s if spread is None else spread + s
    return mean, lax.rsqrt(spread / width + norm_eps)


def shift_down(value, steps, row):
    return jnp.where(row >= steps, pltpu.roll(value, steps, 0), 0.0)


def mixer_kernel(rows, mine_ref, other_ref, small_ref, scale_ref, keep_ref, send_ref, mixed_ref, w_ref):
    x, core = lax.axis_index("x"), lax.axis_index("core")
    for s in range(8):
        for j in range(8):
            w_ref[row_at(core, s, j), :] = small_ref[s, j]
    step = rows // 3
    for t in range(3):
        part = pl.ds(t * step, step)
        blocks = [(ref, r) for ref in (mine_ref, other_ref) for r in range(4)]
        loads = [lambda ref=ref, r=r: ref[r, part, :].astype(f32) for ref, r in blocks]
        mean, inverse = row_statistics(loads, 2048)
        for (ref, r), load in zip(blocks, loads):
            where = columns_of(lax.rem(x + (4 - r), 4), core if ref is mine_ref else 1 - core)
            mixed = (load() - mean) * inverse * gain_of(ref, r, rows, 0)
            mixed_ref[part, where] = mixed.astype(bf16)
    pool_in = jnp.dot(mixed_ref[...], w_ref[:, :128], preferred_element_type=f32)
    u = pool_in.astype(bf16).astype(f32)
    row = lax.broadcasted_iota(jnp.int32, u.shape, 0)
    two = u + shift_down(u, 1, row)
    four = two + shift_down(two, 2, row)
    eight = four + shift_down(four, 4, row)
    sixteen = eight + shift_down(eight, 8, row)
    total = jnp.where(x == 0, two, jnp.where(x == 1, four, jnp.where(x == 2, eight, sixteen)))
    window = jnp.where(x == 0, 2, jnp.where(x == 1, 4, jnp.where(x == 2, 8, 16)))
    count = jnp.minimum(row + 1, window).astype(f32)
    pooled = ((total / count - u) * scale_ref[...]).astype(bf16)
    for xb in range(4):
        for ref, c in ((keep_ref, core), (send_ref, 1 - core)):
            term = lax.dot_general(
                pooled,
                w_ref[columns_of(xb, c), 128:],
                (((1,), (1,)), ((), ())),
                preferred_element_type=f32,
            )
            ref[xb] = term.astype(bf16)


def middle_kernel(rows, mine_ref, other_ref, mix_ref, mix_other_ref, mid_ref, own_ref):
    x, core = lax.axis_index("x"), lax.axis_index("core")
    step = rows // 3
    for t in range(3):
        part = pl.ds(t * step, step)
        blocks = [
            (tok, mix, c, xb)
            for tok, mix, c in ((mine_ref, mix_ref, core), (other_ref, mix_other_ref, 1 - core))
            for xb in range(4)
        ]

        def total(tok, mix, xb):
            r = lax.rem(x + (4 - xb), 4)
            return residual_alpha * tok[r, part, :].astype(f32) + mix[xb, part, :].astype(f32)

        loads = [functools.partial(total, tok, mix, xb) for tok, mix, _, xb in blocks]
        mean, inverse = row_statistics(loads, 2048)
        for (tok, mix, c, xb), load in zip(blocks, loads):
            gain = gain_of(tok, lax.rem(x + (4 - xb), 4), rows, 3)
            mid_ref[part, columns_of(xb, c)] = ((load() - mean) * inverse * gain).astype(bf16)
    own_ref[...] = mid_ref[:, columns_of(x, core)]


def ff_kernel(mid_ref, *refs):
    chunks, (keep_ref, send_ref, hid_ref, w_ref, sems) = refs[:8], refs[8:]
    core = lax.axis_index("core")
    place = jnp.where(core == 0, lax.axis_index("y"), lax.axis_index("z"))
    copies = [[], []]
    for half in range(2):
        where = pl.ds(half * 1024, 1024)
        for k, (chunk, offset) in enumerate(zip(chunks, OFFSETS)):
            source = lax.rem(place + (8 - offset), 8)
            for j in range(8):
                copy = pltpu.make_async_copy(
                    chunk.at[j, :, where],
                    w_ref.at[row_at(core, source, j), where],
                    sems.at[half, k, j],
                )
                copy.start()
                copies[half].append(copy)
    for copy in copies[0]:
        copy.wait()
    for n in range(4):
        where = slice(n * 256, (n + 1) * 256)
        up = jnp.dot(mid_ref[...], w_ref[:, where], preferred_element_type=f32)
        up = jnp.maximum(up, 0.0)
        hid_ref[:, where] = (up * up).astype(bf16)
    for copy in copies[1]:
        copy.wait()
    for xb in range(4):
        for ref, c in ((keep_ref, core), (send_ref, 1 - core)):
            term = lax.dot_general(
                hid_ref[...],
                w_ref[columns_of(xb, c), 1024:],
                (((1,), (1,)), ((), ())),
                preferred_element_type=f32,
            )
            ref[xb] = term.astype(bf16)


def vmem(count):
    return [pl.BlockSpec(memory_space=pltpu.VMEM)] * count


def prepare_kernel(w1_ref, w2_ref, w_in_ref, w_out_ref, blocks_ref):
    for i in range(8):
        blocks_ref[i, :, 0:1024] = w1_ref[...]
        blocks_ref[i, :, 1024:2048] = w2_ref[...]
        blocks_ref[i, :, 2048:2176] = w_in_ref[...]
        blocks_ref[i, :, 2176:2304] = w_out_ref[...]


def add_kernel(one_ref, other_ref, out_ref):
    for i in range(4):
        out_ref[i] = (one_ref[i].astype(f32) + other_ref[i].astype(f32)).astype(bf16)


def spread_kernel(four_ref, out_ref):
    low = four_ref[0].astype(f32) + four_ref[1].astype(f32)
    high = four_ref[2].astype(f32) + four_ref[3].astype(f32)
    total = (low + high).astype(bf16)
    for i in range(4):
        out_ref[i] = total


def small_kernel(kernel, shape, *operands):
    return pl.pallas_call(
        kernel,
        out_shape=jax.ShapeDtypeStruct(shape, bf16),
        in_specs=vmem(len(operands)),
        out_specs=vmem(1)[0],
        compiler_params=pltpu.CompilerParams(vmem_limit_bytes=8 * MEBI),
        cost_estimate=pl.CostEstimate(flops=1_000_000, bytes_accessed=2_000_000, transcendentals=0),
    )(*operands)


def split_kernel(first_ref, chunk_ref, blocks_ref, small_ref, sems):
    small = pltpu.make_async_copy(first_ref.at[:, :, pl.ds(2048, 256)], small_ref, sems.at[0])
    chunk = pltpu.make_async_copy(first_ref.at[:, :, pl.ds(0, 2048)], chunk_ref, sems.at[1])
    small.start()
    chunk.start()
    small.wait()
    rows = small_ref[...].reshape(256, 256)
    for i in range(8):
        blocks_ref[i] = rows
    chunk.wait()


def split(first):
    return pl.pallas_call(
        split_kernel,
        out_shape=(
            jax.ShapeDtypeStruct((8, 32, 2048), bf16),
            jax.ShapeDtypeStruct((8, 256, 256), bf16),
        ),
        in_specs=[pl.BlockSpec(memory_space=pl.ANY)],
        out_specs=tuple(vmem(2)),
        scratch_shapes=[pltpu.VMEM((8, 32, 256), bf16), pltpu.SemaphoreType.DMA((2,))],
        compiler_params=pltpu.CompilerParams(vmem_limit_bytes=8 * MEBI),
        cost_estimate=pl.CostEstimate(flops=1_000_000, bytes_accessed=3_000_000, transcendentals=0),
        name="split",
    )(first)


def mixer(mine, other, small, scale, rows, width, channels):
    block = jax.ShapeDtypeStruct((4, rows, width), bf16)
    return pl.pallas_call(
        functools.partial(mixer_kernel, rows),
        out_shape=(block, block),
        in_specs=vmem(4),
        out_specs=tuple(vmem(2)),
        scratch_shapes=[
            pltpu.VMEM((rows, 8 * width), bf16),
            pltpu.VMEM((8 * width, 2 * channels), bf16),
        ],
        compiler_params=pltpu.CompilerParams(vmem_limit_bytes=24 * MEBI),
        cost_estimate=pl.CostEstimate(flops=4_000_000_000, bytes_accessed=4_000_000, transcendentals=0),
        name="mixer",
    )(mine, other, small, scale)


def middle_of(mine, other, mix, mix_other, rows, width):
    return pl.pallas_call(
        functools.partial(middle_kernel, rows),
        out_shape=(
            jax.ShapeDtypeStruct((rows, 8 * width), bf16),
            jax.ShapeDtypeStruct((rows, width), bf16),
        ),
        in_specs=vmem(4),
        out_specs=tuple(vmem(2)),
        compiler_params=pltpu.CompilerParams(vmem_limit_bytes=16 * MEBI),
        cost_estimate=pl.CostEstimate(flops=2_000_000_000, bytes_accessed=5_000_000, transcendentals=0),
        name="middle",
    )(mine, other, mix, mix_other)


def feed_forward(full, chunks, rows, width):
    block = jax.ShapeDtypeStruct((4, rows, width), bf16)
    return pl.pallas_call(
        ff_kernel,
        out_shape=(block, block),
        in_specs=vmem(1) + [pl.BlockSpec(memory_space=pl.ANY)] * 8,
        out_specs=tuple(vmem(2)),
        scratch_shapes=[
            pltpu.VMEM((rows, 1024), bf16),
            pltpu.VMEM((2048, 2048), bf16),
            pltpu.SemaphoreType.DMA((2, 8, 8)),
        ],
        compiler_params=pltpu.CompilerParams(vmem_limit_bytes=30 * MEBI),
        cost_estimate=pl.CostEstimate(flops=6_000_000_000, bytes_accessed=12_000_000, transcendentals=0),
        name="feed_forward",
    )(full, *chunks)


def layer(tokens, gain_mixer, w_in, pool_scale, w_pool_out, gain_mid, w_ff1, w_ff2, gain_out):
    rows, width = tokens.shape
    channels = w_in.shape[1]
    weights = (w_ff1, w_ff2, w_in, w_pool_out)
    packed = small_kernel(prepare_kernel, (8, 32, 2304), *weights)
    first = exchanged(packed, FIRST)
    chunk, blocks = split(first)
    small = exchanged(blocks, SECOND)
    small = small.reshape(8, 8, 32, 2 * channels)
    chunks = [chunk]
    up, down = chunk, chunk
    for hop in range(4):
        down = lax.ppermute(down, EVERY, around(-1))
        chunks.append(down)
        if hop < 3:
            up = lax.ppermute(up, EVERY, around(1))
            chunks.append(up)
    extended = jnp.concatenate(
        [tokens, in_three(gain_mixer), in_three(gain_mid), jnp.zeros((10, width), bf16)]
    )
    pieces = [extended]
    for steps in (1, 2, 3):
        pieces.append(along_x(extended, steps))
    mine = jnp.stack(pieces)
    other = from_other_core(mine)
    keep, send = mixer(mine, other, small, pool_scale[None], rows, width, channels)
    block = (4, rows, width)
    chip = small_kernel(add_kernel, block, keep, from_other_core(send))
    four = lax.all_to_all(chip, "x", 0, 0, tiled=True)
    spread = small_kernel(spread_kernel, block, four)
    mix = lax.all_to_all(spread, "x", 0, 0, tiled=True)
    mix_other = from_other_core(mix)
    full, middle = middle_of(mine, other, mix, mix_other, rows, width)
    keep, send = feed_forward(full, chunks, rows, width)
    ff_out = scatter_sum_tp(keep, send).astype(bf16)
    value = residual_alpha * middle.astype(f32) + ff_out.astype(f32)
    part_mean = jnp.sum(value, axis=1) / width
    center = value - part_mean[:, None]
    part_spread = jnp.sum(center * center, axis=1)
    sums = jnp.concatenate([part_mean, part_spread])[None]
    means, spreads = jnp.split(everyone(sums, TP)[:, 0], 2, axis=1)
    mean = jnp.mean(means, axis=0)
    away = means - mean
    spread = (jnp.sum(spreads, axis=0) + width * jnp.sum(away * away, axis=0)) / (8 * width)
    result = (value - mean[:, None]) * lax.rsqrt(spread + norm_eps)[:, None] * gain_out
    return result.astype(bf16)


def solution(mesh):
    mesh = Mesh(mesh.devices.reshape(8, 8, 4, 2), EVERY)
    return jax.shard_map(
        layer,
        mesh=mesh,
        in_specs=(
            P(FS, TP),
            P(TP),
            P(FS, TP),
            P(TP),
            P(FS, TP),
            P(TP),
            P(FS, TP),
            P(FS, TP),
            P(TP),
        ),
        out_specs=P(FS, TP),
        check_vma=False,
    )
```

```python
import functools

import jax
import jax.numpy as jnp
from jax import lax
from jax.experimental import pallas as pl
from jax.experimental.pallas import tpu as pltpu
from jax.sharding import Mesh, PartitionSpec as P


norm_eps = 1e-05
residual_alpha = 2.0**0.25
FS = ("z", "y")
TP = ("x", "core")
EVERY = FS + TP
bf16 = jnp.bfloat16
f32 = jnp.float32
OFFSETS = (0, -1, 1, -2, 2, -3, 3, -4)
MEBI = 1024 * 1024


def device(z, y, x, core):
    return (((z % 8) * 8 + y % 8) * 4 + x % 4) * 2 + core % 2


PLACES = [(z, y, x) for z in range(8) for y in range(8) for x in range(4)]
FIRST = [[device(z, y, x, 0) for z in range(8)] for y in range(8) for x in range(4)] + [
    [device(z, y, x, 1) for y in range(8)] for z in range(8) for x in range(4)
]
SECOND = [[device(z, y, x, 0) for y in range(8)] for z in range(8) for x in range(4)] + [
    [device(z, y, x, 1) for z in range(8)] for y in range(8) for x in range(4)
]


def around(steps):
    return [
        pair
        for z, y, x in PLACES
        for pair in (
            (device(z, y, x, 0), device(z, y + steps, x, 0)),
            (device(z, y, x, 1), device(z + steps, y, x, 1)),
        )
    ]


def along_x(array, steps):
    pairs = [
        (device(z, y, x, c), device(z, y, x + steps, c)) for z, y, x in PLACES for c in range(2)
    ]
    return lax.ppermute(array, EVERY, pairs)


def from_other_core(array):
    return lax.ppermute(array, "core", [(0, 1), (1, 0)])


def everyone(array, axis):
    count = lax.axis_size(axis)
    return lax.all_to_all(
        jnp.broadcast_to(array[None], (count, *array.shape)), axis, 0, 0, tiled=True
    )


def among(array, groups):
    return lax.all_to_all(
        jnp.broadcast_to(array[None], (8, *array.shape)),
        EVERY,
        0,
        0,
        axis_index_groups=groups,
        tiled=True,
    )


def scatter_sum_tp(keep, send):
    chip = (keep.astype(f32) + from_other_core(send).astype(f32)).astype(bf16)
    four = lax.all_to_all(chip, "x", 0, 0, tiled=True).astype(f32)
    return (four[0] + four[1]) + (four[2] + four[3])


def in_three(gain):
    rest, rows = gain, []
    for _ in range(3):
        rows.append(lax.reduce_precision(rest, 8, 7))
        rest = rest - rows[-1]
    return jnp.stack(rows).astype(bf16)


def gain_of(tok_ref, block, rows, first):
    parts = tok_ref[block, pl.ds(rows, 16), :].astype(f32)
    return parts[first : first + 1] + parts[first + 1 : first + 2] + parts[first + 2 : first + 3]


def columns_of(x, core):
    return pl.ds(pl.multiple_of((2 * x + core) * 256, 256), 256)


def row_at(core, source, j):
    at = jnp.where(core == 0, j * 256 + source * 32, source * 256 + j * 32)
    return pl.ds(pl.multiple_of(at, 32), 32)


def row_statistics(loads, width):
    total = None
    for load in loads:
        s = jnp.sum(load(), axis=1, keepdims=True)
        total = s if total is None else total + s
    mean = total / width
    spread = None
    for load in loads:
        c = load() - mean
        s = jnp.sum(c * c, axis=1, keepdims=True)
        spread = s if spread is None else spread + s
    return mean, lax.rsqrt(spread / width + norm_eps)


def shift_down(value, steps, row):
    return jnp.where(row >= steps, pltpu.roll(value, steps, 0), 0.0)


def mixer_kernel(rows, mine_ref, other_ref, small_ref, scale_ref, keep_ref, send_ref, mixed_ref, w_ref):
    x, core = lax.axis_index("x"), lax.axis_index("core")
    for s in range(8):
        for j in range(8):
            w_ref[row_at(core, s, j), :] = small_ref[s, j]
    step = rows // 3
    for t in range(3):
        part = pl.ds(t * step, step)
        blocks = [(ref, r) for ref in (mine_ref, other_ref) for r in range(4)]
        loads = [lambda ref=ref, r=r: ref[r, part, :].astype(f32) for ref, r in blocks]
        mean, inverse = row_statistics(loads, 2048)
        for (ref, r), load in zip(blocks, loads):
            where = columns_of(lax.rem(x + (4 - r), 4), core if ref is mine_ref else 1 - core)
            mixed = (load() - mean) * inverse * gain_of(ref, r, rows, 0)
            mixed_ref[part, where] = mixed.astype(bf16)
    pool_in = jnp.dot(mixed_ref[...], w_ref[:, :128], preferred_element_type=f32)
    u = pool_in.astype(bf16).astype(f32)
    row = lax.broadcasted_iota(jnp.int32, u.shape, 0)
    two = u + shift_down(u, 1, row)
    four = two + shift_down(two, 2, row)
    eight = four + shift_down(four, 4, row)
    sixteen = eight + shift_down(eight, 8, row)
    total = jnp.where(x == 0, two, jnp.where(x == 1, four, jnp.where(x == 2, eight, sixteen)))
    window = jnp.where(x == 0, 2, jnp.where(x == 1, 4, jnp.where(x == 2, 8, 16)))
    count = jnp.minimum(row + 1, window).astype(f32)
    pooled = ((total / count - u) * scale_ref[...]).astype(bf16)
    for xb in range(4):
        for ref, c in ((keep_ref, core), (send_ref, 1 - core)):
            term = lax.dot_general(
                pooled,
                w_ref[columns_of(xb, c), 128:],
                (((1,), (1,)), ((), ())),
                preferred_element_type=f32,
            )
            ref[xb] = term.astype(bf16)


def middle_kernel(rows, mine_ref, other_ref, mix_ref, mix_other_ref, mid_ref, own_ref):
    x, core = lax.axis_index("x"), lax.axis_index("core")
    step = rows // 3
    for t in range(3):
        part = pl.ds(t * step, step)
        blocks = [
            (tok, mix, c, xb)
            for tok, mix, c in ((mine_ref, mix_ref, core), (other_ref, mix_other_ref, 1 - core))
            for xb in range(4)
        ]

        def total(tok, mix, xb):
            r = lax.rem(x + (4 - xb), 4)
            return residual_alpha * tok[r, part, :].astype(f32) + mix[xb, part, :].astype(f32)

        loads = [functools.partial(total, tok, mix, xb) for tok, mix, _, xb in blocks]
        mean, inverse = row_statistics(loads, 2048)
        for (tok, mix, c, xb), load in zip(blocks, loads):
            gain = gain_of(tok, lax.rem(x + (4 - xb), 4), rows, 3)
            mid_ref[part, columns_of(xb, c)] = ((load() - mean) * inverse * gain).astype(bf16)
    own_ref[...] = mid_ref[:, columns_of(x, core)]


def ff_kernel(mid_ref, *refs):
    chunks, (keep_ref, send_ref, hid_ref, w_ref, sems) = refs[:8], refs[8:]
    core = lax.axis_index("core")
    place = jnp.where(core == 0, lax.axis_index("y"), lax.axis_index("z"))
    groups = [pl.ds(n * 256, 256) for n in range(4)] + [pl.ds(1024, 1024)]

    def copies(g, along_y):
        result = []
        for k, (chunk, offset) in enumerate(zip(chunks, OFFSETS)):
            source = lax.rem(place + (8 - offset), 8)
            if along_y:
                target = w_ref.at[:, source, :, groups[g]]
            else:
                target = w_ref.at[source, :, :, groups[g]]
            result.append(
                pltpu.make_async_copy(chunk.at[:, :, groups[g]], target, sems.at[g, k])
            )
        return result

    @pl.when(core == 0)
    def _():
        for g in range(5):
            for copy in copies(g, True):
                copy.start()

    @pl.when(core == 1)
    def _():
        for g in range(5):
            for copy in copies(g, False):
                copy.start()

    for n in range(4):
        for copy in copies(n, False):
            copy.wait()
        w_up = w_ref[:, :, :, n * 256 : (n + 1) * 256].reshape(2048, 256)
        up = jnp.dot(mid_ref[...], w_up, preferred_element_type=f32)
        up = jnp.maximum(up, 0.0)
        hid_ref[:, n * 256 : (n + 1) * 256] = (up * up).astype(bf16)
    for copy in copies(4, False):
        copy.wait()
    for xb in range(4):
        for ref, c in ((keep_ref, core), (send_ref, 1 - core)):
            term = lax.dot_general(
                hid_ref[...],
                w_ref[2 * xb + c, :, :, 1024:].reshape(256, 1024),
                (((1,), (1,)), ((), ())),
                preferred_element_type=f32,
            )
            ref[xb] = term.astype(bf16)


def vmem(count):
    return [pl.BlockSpec(memory_space=pltpu.VMEM)] * count


def mixer(mine, other, small, scale, rows, width, channels):
    block = jax.ShapeDtypeStruct((4, rows, width), bf16)
    return pl.pallas_call(
        functools.partial(mixer_kernel, rows),
        out_shape=(block, block),
        in_specs=vmem(4),
        out_specs=tuple(vmem(2)),
        scratch_shapes=[
            pltpu.VMEM((rows, 8 * width), bf16),
            pltpu.VMEM((8 * width, 2 * channels), bf16),
        ],
        compiler_params=pltpu.CompilerParams(vmem_limit_bytes=24 * MEBI),
        cost_estimate=pl.CostEstimate(flops=4_000_000_000, bytes_accessed=4_000_000, transcendentals=0),
        name="mixer",
    )(mine, other, small, scale)


def middle_of(mine, other, mix, mix_other, rows, width):
    return pl.pallas_call(
        functools.partial(middle_kernel, rows),
        out_shape=(
            jax.ShapeDtypeStruct((rows, 8 * width), bf16),
            jax.ShapeDtypeStruct((rows, width), bf16),
        ),
        in_specs=vmem(4),
        out_specs=tuple(vmem(2)),
        compiler_params=pltpu.CompilerParams(vmem_limit_bytes=16 * MEBI),
        cost_estimate=pl.CostEstimate(flops=2_000_000_000, bytes_accessed=5_000_000, transcendentals=0),
        name="middle",
    )(mine, other, mix, mix_other)


def feed_forward(full, chunks, rows, width):
    block = jax.ShapeDtypeStruct((4, rows, width), bf16)
    return pl.pallas_call(
        ff_kernel,
        out_shape=(block, block),
        in_specs=vmem(1) + [pl.BlockSpec(memory_space=pl.ANY)] * 8,
        out_specs=tuple(vmem(2)),
        scratch_shapes=[
            pltpu.VMEM((rows, 1024), bf16),
            pltpu.VMEM((8, 8, 32, 2048), bf16),
            pltpu.SemaphoreType.DMA((5, 8)),
        ],
        compiler_params=pltpu.CompilerParams(vmem_limit_bytes=30 * MEBI),
        cost_estimate=pl.CostEstimate(flops=6_000_000_000, bytes_accessed=12_000_000, transcendentals=0),
        name="feed_forward",
    )(full, *chunks)


def layer(tokens, gain_mixer, w_in, pool_scale, w_pool_out, gain_mid, w_ff1, w_ff2, gain_out):
    rows, width = tokens.shape
    channels = w_in.shape[1]
    packed = jnp.concatenate([w_ff1, w_ff2, w_in, w_pool_out], axis=1)
    first = among(packed, FIRST)
    small = among(first[:, :, 2048:].reshape(256, 2 * channels), SECOND)
    small = small.reshape(8, 8, 32, 2 * channels)
    chunk = first[:, :, :2048]
    chunks = [chunk]
    up, down = chunk, chunk
    for hop in range(4):
        down = lax.ppermute(down, EVERY, around(-1))
        chunks.append(down)
        if hop < 3:
            up = lax.ppermute(up, EVERY, around(1))
            chunks.append(up)
    extended = jnp.concatenate(
        [tokens, in_three(gain_mixer), in_three(gain_mid), jnp.zeros((10, width), bf16)]
    )
    pieces = [extended]
    for steps in (1, 2, 3):
        pieces.append(along_x(extended, steps))
    mine = jnp.stack(pieces)
    other = from_other_core(mine)
    keep, send = mixer(mine, other, small, pool_scale[None], rows, width, channels)
    mixer_out = scatter_sum_tp(keep, send).astype(bf16)
    mix = everyone(mixer_out, "x")
    mix_other = from_other_core(mix)
    full, middle = middle_of(mine, other, mix, mix_other, rows, width)
    keep, send = feed_forward(full, chunks, rows, width)
    ff_out = scatter_sum_tp(keep, send).astype(bf16)
    value = residual_alpha * middle.astype(f32) + ff_out.astype(f32)
    part_mean = jnp.sum(value, axis=1) / width
    center = value - part_mean[:, None]
    part_spread = jnp.sum(center * center, axis=1)
    sums = jnp.concatenate([part_mean, part_spread])[None]
    means, spreads = jnp.split(everyone(sums, TP)[:, 0], 2, axis=1)
    mean = jnp.mean(means, axis=0)
    away = means - mean
    spread = (jnp.sum(spreads, axis=0) + width * jnp.sum(away * away, axis=0)) / (8 * width)
    result = (value - mean[:, None]) * lax.rsqrt(spread + norm_eps)[:, None] * gain_out
    return result.astype(bf16)


def solution(mesh):
    mesh = Mesh(mesh.devices.reshape(8, 8, 4, 2), EVERY)
    return jax.shard_map(
        layer,
        mesh=mesh,
        in_specs=(
            P(FS, TP),
            P(TP),
            P(FS, TP),
            P(TP),
            P(FS, TP),
            P(TP),
            P(FS, TP),
            P(FS, TP),
            P(TP),
        ),
        out_specs=P(FS, TP),
        check_vma=False,
    )
```
